256 devices in a mesh: fs: 32 (over z, x), tp: 8 (over y, core).
Axes of the slice: x: 4, y: 4, z: 8, core: 2. Of those that a mesh axis runs over, the one named last changes fastest.
Arguments:
- tokens: bfloat16 [1280, 4096], P('fs'), may hold values from -6 to 6
- routes: int32 [1280, 2], P('fs'), may hold values from 0 to 3, all different within a row; in each aligned block of 40 rows (0 to 39, 40 to 79, ...) at most 30 rows name the same one
- route_logits: float32 [1280, 2], P('fs'), may hold values from -6 to 6
- norm_gain: float32 [4096], P('fs'), may hold values from 0.1 to 1.9
- gate_weight: float32 [4, 4096, 8192], P(None, 'fs', 'tp'), may hold values from -0.09375 to 0.09375
- up_weight: float32 [4, 4096, 8192], P(None, 'fs', 'tp'), may hold values from -0.09375 to 0.09375
- down_weight: float32 [4, 4096, 8192], P(None, 'fs', 'tp'), may hold values from -0.0625 to 0.0625
Outputs:
- mixed: bfloat16 [1280, 4096], P('fs', 'tp')
- gate_sampler: bfloat16 [8, 4096, 4096], P('tp', None, 'fs')
- up_sampler: bfloat16 [8, 4096, 4096], P('tp', None, 'fs')
- down_sampler: bfloat16 [8, 4096, 4096], P('tp', None, 'fs')
The draws below stay inside these ranges and needn't reach their ends.
Inputs may be any that keep to these rules, and one draw needn't show every extreme that they name: `routes`: the 2 experts of a token differ. Within the tokens of one index of fs (aligned blocks of 40 rows) no expert is named by more than 30 tokens.
All inputs are finite; a program needn't handle non-finite values.
Results may differ from the reference program's by a relative error of at most 0.01.
Values may be sent and summed in bfloat16 or wider, within the bound.
A program may use at most 128 MiB of HBM per device.

```python
import math
import jax
import jax.numpy as jnp
import numpy as np
from jax import lax

D = 4096
FF = 8192
EXPERTS = 4
TOPK = 2
TOK_DEV = 40
CAP = 30
TOKENS = 1280
N_TP = 8


def block_scale(own_key, extent, pieces, least, high):
    gain = 1.0
    for dim, parts in pieces:
        heights = jax.random.uniform(jax.random.fold_in(jax.random.fold_in(own_key, 6), dim), (parts,), jnp.float32, least / len(pieces), high / len(pieces))
        gain = gain * jnp.repeat(jnp.exp(heights), extent[dim] // parts).reshape((-1,) + (1,) * (len(extent) - 1 - dim))
    return gain


def assign_block(own_key, own, number, rows, number_of, top, limit, lean):
    order = jax.random.permutation(own_key, number_of)
    heavy_load, usual = portions_of(number_of, rows * top, limit, lean, True), portions_of(number_of, rows * top, limit, lean, False)
    places = jnp.arange(number_of)

    def named(sizes, offset_by):
        used = int((sizes > 0).sum())
        fixed = max(1, used // 4)
        moved = fixed + (places - fixed + offset_by * (used - fixed)) % max(1, number_of - fixed)
        return jnp.zeros((number_of,), jnp.int32).at[order[jnp.where(places < fixed, places, moved)]].set(jnp.asarray(sizes, jnp.int32))

    sizes = jnp.where(number % 4 == 0, named(heavy_load, number // 4), named(usual, number - number // 4 - 1))
    mixed = jax.random.permutation(jax.random.fold_in(own, 3), number_of)
    donor, sink = mixed[0:number_of // 2 * 2:2], mixed[1:number_of // 2 * 2:2]
    room = jnp.minimum(sizes[donor] - 1, limit - sizes[sink]) // 2
    room = jnp.where((donor == order[0]) | (sink == order[0]) | (sizes[sink] == 0), 0, jnp.maximum(room, 0))
    moved = jax.random.randint(jax.random.fold_in(own, 4), (number_of // 2,), 0, 1 << 20) % (room + 1)
    sizes = sizes.at[donor].add(-moved).at[sink].add(moved)
    labels = jnp.searchsorted(jnp.cumsum(sizes), jnp.arange(rows * top), side="right").astype(jnp.int32)
    grid = labels.reshape(top, rows).T
    grid = grid[jax.random.permutation(jax.random.fold_in(own, 1), rows)]
    offset_by = jax.random.randint(jax.random.fold_in(own, 2), (rows, 1), 0, top)
    return jnp.take_along_axis(grid, (jnp.arange(top)[None, :] + offset_by) % top, axis=1)


def portions_of(count, total, most, slope, full):
    loads = [(1 << 20) // math.isqrt(rank ** slope) + 1 for rank in range(1, count + 1)]
    largest = most if full else min(most, max(-(-total // count), total * loads[0] // sum(loads)))
    least = 1 if total - largest >= count - 1 else 0
    holding, spare = [largest] + [least] * (count - 1), total - largest - least * (count - 1)
    while spare > 0:
        free = [i for i in range(1, count) if holding[i] < largest] or [i for i in range(1, count) if holding[i] < most]
        mass, remaining = sum([loads[i] for i in free]), spare
        for i in free:
            extra = min(most - holding[i], max(1, remaining * loads[i] // mass), spare)
            holding[i] = holding[i] + extra
            spare = spare - extra
    return np.array(holding)


def centred(key, extent, scale, reach, cuts=(), held_as=jnp.bfloat16):
    drawn = jax.random.normal(key, extent, jnp.float32) * scale
    if len(cuts) > 0:
        drawn = block_scale(key, extent, cuts, -0.22, 0.18) * drawn
    return jnp.clip(drawn, min=-reach, max=reach).astype(held_as)


def setup_inputs(seed: int = 0) -> dict:
    arg_keys = jax.random.split(jax.random.key(seed), 8)
    tokens = centred(arg_keys[0], (TOKENS, D), 1.0, 6.0, ((0, 32),))
    routes_keys = jax.random.split(jax.random.fold_in(arg_keys[1], 1), TOKENS // TOK_DEV)
    routes_turns = jax.random.permutation(jax.random.fold_in(arg_keys[1], 3), TOKENS // TOK_DEV)
    routes = jax.vmap(lambda own, number: assign_block(jax.random.fold_in(arg_keys[1], 2), own, number, TOK_DEV, EXPERTS, TOPK, CAP, 2))(routes_keys, routes_turns).reshape((TOKENS, TOPK))
    route_logits = centred(arg_keys[2], (TOKENS, TOPK), 1.5, 6.0, ((0, 32),), jnp.float32)
    norm_gain = jnp.clip(1.0 + 0.18 * jax.random.normal(arg_keys[3], (D,), jnp.float32), 0.1, 1.9)
    gate_weight = centred(arg_keys[4], (EXPERTS, D, FF), D ** -0.5, 0.09375, ((1, 32), (2, 8)), jnp.float32)
    up_weight = centred(arg_keys[5], (EXPERTS, D, FF), D ** -0.5, 0.09375, ((1, 32), (2, 8)), jnp.float32)
    down_weight = centred(arg_keys[6], (EXPERTS, D, FF), FF ** -0.5, 0.0625, ((1, 32), (2, 8)), jnp.float32)
    return {"tokens": tokens, "routes": routes, "route_logits": route_logits, "norm_gain": norm_gain, "gate_weight": gate_weight, "up_weight": up_weight, "down_weight": down_weight}


def arrange(matrix):
    experts, width, hidden_units = matrix.shape
    block = hidden_units // N_TP
    split = matrix.reshape(experts, width, N_TP, block)
    return jnp.transpose(split, (2, 1, 0, 3)).reshape(N_TP, width, experts * block)

def reference(tokens, routes, route_logits, norm_gain, gate_weight, up_weight, down_weight):
    gain_cols = norm_gain.astype(jnp.float32)[None, :, None]
    folded_gate = (gate_weight * gain_cols).astype(jnp.bfloat16)
    folded_up = (up_weight * gain_cols).astype(jnp.bfloat16)
    rounded_down = down_weight.astype(jnp.bfloat16)
    tok_float = tokens.astype(jnp.float32)
    normed = (tok_float * lax.rsqrt(lax.optimization_barrier(jnp.mean(tok_float * tok_float, axis=1, keepdims=True)) + 1e-05)).astype(jnp.bfloat16)
    shares = jax.nn.sigmoid(route_logits - route_logits[:, ::-1])
    mixed = jnp.zeros((tokens.shape[0], tokens.shape[1]), jnp.float32)
    for expert in range(EXPERTS):
        gate_act = jnp.dot(normed, folded_gate[expert], preferred_element_type=jnp.float32)
        up_act = jnp.dot(normed, folded_up[expert], preferred_element_type=jnp.float32)
        hidden = (jax.nn.silu(gate_act) * up_act).astype(jnp.bfloat16)
        expert_out = lax.dot_general(hidden, rounded_down[expert], (((1,), (1,)), ((), ())), preferred_element_type=jnp.float32)
        weight = lax.optimization_barrier(jnp.sum(jnp.where(routes == expert, shares, 0.0), axis=1))
        mixed = mixed + weight[:, None] * expert_out
    return (mixed.astype(jnp.bfloat16), arrange(folded_gate), arrange(folded_up), arrange(rounded_down))
```

```python
import functools

import jax
import jax.numpy as jnp
from jax import lax
from jax.experimental import pallas as pl
from jax.experimental.pallas import tpu as pltpu
from jax.sharding import PartitionSpec as P

MESH = pl.DeviceIdType.MESH
NZ, NX, NY = 8, 4, 4
NFS, NTP = 32, 8
EXPERTS = 4
D = 4096
KB = D // NTP
TOK = 40
SLOT = 32
ROWS = NFS * SLOT
XROWS = NZ * SLOT
NC = 4
DR = 128 // NC
CW = NX * DR
F32, BF16 = jnp.float32, jnp.bfloat16


def rem(a, n):
    return lax.rem(a, jnp.int32(n))


def div(a, n):
    return lax.div(a, jnp.int32(n))


def kernel(
    tok_hbm, routes_ref, logits_ref, gain_ref, gate_hbm, up_hbm, down_hbm,
    mixed_ref, gate_out, up_out, down_out,
    tok, stage, wmix, p_send, sg, sd, wgu, wd, xg, hid, dn, ro, r1, r2, rr,
    tok_sem, load_sem,
    t1_s, t1_r, t2_s, t2_r, t3_s, t3_r, t3f_s, cc_s, cc_r,
    gu_s, gu_r, wd_s, wd_r, h_s, h_r, hc_s, hc_r, dn_s, dn_r, r1_s, r1_r, r2_s, r2_r,
    out_sem, outd_sem,
):
    fs, tp = lax.axis_index("fs"), lax.axis_index("tp")
    z, x = div(fs, NX), rem(fs, NX)
    y, core = div(tp, 2), rem(tp, 2)

    def rcopy(src, dst, ssem, rsem, fs2, tp2):
        return pltpu.make_async_remote_copy(
            src_ref=src, dst_ref=dst, send_sem=ssem, recv_sem=rsem,
            device_id=(fs2, tp2), device_id_type=MESH,
        )

    def wait_for(sem, ref):
        pltpu.make_async_copy(ref, ref, sem).wait()

    def tp_of(dy):
        return rem(y + dy, NY) * 2 + core

    other = y * 2 + (1 - core)

    bar = pltpu.get_barrier_semaphore()

    @pl.loop(1, NFS)
    def _(i):
        pl.semaphore_signal(bar, inc=1, device_id=(rem(fs + i, NFS), tp), device_id_type=MESH)

    @pl.loop(1, NTP)
    def _(i):
        pl.semaphore_signal(bar, inc=1, device_id=(fs, rem(tp + i, NTP)), device_id_type=MESH)

    tok_copy = pltpu.make_async_copy(tok_hbm, tok, tok_sem)
    tok_copy.start()
    loads = []
    for m, hbm in enumerate((gate_hbm, up_hbm, down_hbm)):
        cp = pltpu.make_async_copy(hbm, stage.at[m], load_sem.at[m])
        cp.start()
        loads.append(cp)

    lane = lax.broadcasted_iota(jnp.int32, (TOK, EXPERTS * SLOT), 1)
    lane_e = div(lane, SLOT)
    lane_s = rem(lane, SLOT).astype(F32)
    pick0 = jnp.where(routes_ref[:, 0:1] == lane_e, 1.0, 0.0).astype(F32)
    pick1 = jnp.where(routes_ref[:, 1:2] == lane_e, 1.0, 0.0).astype(F32)
    member = pick0 + pick1
    row_i = lax.broadcasted_iota(jnp.int32, (TOK, TOK), 0)
    col_i = lax.broadcasted_iota(jnp.int32, (TOK, TOK), 1)
    before = jnp.where(col_i < row_i, 1.0, 0.0).astype(BF16)
    position = jnp.dot(before, member.astype(BF16), preferred_element_type=F32)
    placing = jnp.where((position == lane_s) & (member > 0.0), 1.0, 0.0).astype(F32)
    diff = logits_ref[:, 0:1] - logits_ref[:, 1:2]
    share0 = 1.0 / (1.0 + jnp.exp(-diff))
    share1 = 1.0 / (1.0 + jnp.exp(diff))
    wmix[...] = placing * (pick0 * share0 + pick1 * share1)

    tok_copy.wait()
    tf = tok[...].astype(F32)
    inv = lax.rsqrt(jnp.mean(tf * tf, axis=1, keepdims=True) + 1e-05)
    block = tok[:, pl.ds(pl.multiple_of(tp * KB, KB), KB)].astype(F32)
    normed = (block * inv).astype(BF16)
    packed = lax.dot_general(
        placing.astype(BF16), normed, (((0,), (0,)), ((), ())), preferred_element_type=F32
    )
    p_send[...] = packed.astype(BF16).reshape(EXPERTS, SLOT, KB)
    own_x = pl.multiple_of(x * XROWS, XROWS)
    own_row = pl.multiple_of(x * XROWS + z * SLOT, SLOT)
    xg[tp, pl.ds(own_row, SLOT), :] = p_send[div(z, 2)]

    gain = jnp.transpose(jnp.broadcast_to(gain_ref[...], (128, 128)))
    for m in range(2):
        loads[m].wait()

        @pl.loop(0, EXPERTS)
        def _(e):
            for s in range(8):
                sg[e * 8 + s, :, m * 128 : (m + 1) * 128] = (
                    stage[m, e, :, s * 128 : (s + 1) * 128] * gain
                ).astype(BF16)

    wgu[pl.ds(pl.multiple_of(fs * 128, 128), 128), :] = sg[fs]

    pl.semaphore_wait(bar, NFS - 1 + NTP - 1)

    @pl.loop(1, NZ)
    def _(dz):
        z2 = rem(z + dz, NZ)
        rcopy(
            p_send.at[div(z2, 2)], xg.at[tp, pl.ds(own_row, SLOT), :], t1_s, t1_r, z2 * NX + x, tp
        ).start()

    my_rows = pl.ds(pl.multiple_of(fs * 128, 128), 128)

    def send_gu(dz, dx):
        f2 = rem(z + dz, NZ) * NX + rem(x + dx, NX)
        rcopy(sg.at[f2], wgu.at[my_rows, :], gu_s, gu_r, f2, tp).start()

    def send_down(k, i):
        dx, dz = div(i, NZ), rem(i, NZ)
        f2 = rem(z + dz, NZ) * NX + rem(x + dx, NX)
        part = pl.ds(k * DR, DR)
        rcopy(
            sd.at[f2, part, :], wd.at[z, x, part, :], wd_s.at[k], wd_r.at[k], f2, tp
        ).start()

    @pl.loop(1, NZ)
    def _(dz):
        send_gu(dz, 0)

    loads[2].wait()

    @pl.loop(0, EXPERTS)
    def _(e):
        for s in range(8):
            sd[e * 8 + s] = stage[2, e, :, s * 128 : (s + 1) * 128].astype(BF16)

    wd[z, x] = sd[fs]

    wait_for(t1_r, xg.at[0, 0 : (NZ - 1) * SLOT, :])
    mine = xg.at[tp, pl.ds(own_x, XROWS), :]
    t2 = []
    for dx in range(1, NX):
        cp = rcopy(mine, mine, t2_s.at[dx - 1], t2_r.at[dx - 1], z * NX + rem(x + dx, NX), tp)
        cp.start()
        t2.append(cp)

    def part_of(t, p, half=None):
        base = rem(x + NX - p, NX) * XROWS
        if half is None:
            return xg.at[t, pl.ds(pl.multiple_of(base, XROWS), XROWS), :]
        h = XROWS // 2
        return xg.at[t, pl.ds(pl.multiple_of(base + half * h, h), h), :]

    def to_core(t, p):
        ref = part_of(t, p)
        rcopy(ref, ref, cc_s, cc_r, fs, other).start()

    def own_part(p):
        ref = part_of(tp, p)
        rcopy(ref, ref, t3_s, t3_r.at[0, p], fs, tp_of(1)).start()
        rcopy(ref, ref, t3_s, t3_r.at[1, p], fs, tp_of(3)).start()
        to_core(tp, p)

    own_part(0)

    @pl.loop(0, 3 * NZ)
    def _(i):
        send_gu(rem(i, NZ), 1 + div(i, NZ))

    for k in range(min(2, NC)):

        @pl.loop(1, NFS)
        def _(i):
            send_down(k, i)

    for p in range(1, NX):
        t2[p - 1].wait_recv()
        own_part(p)

    for p in range(NX):
        below, above = tp_of(3), tp_of(1)
        ref = part_of(below, p)
        wait_for(t3_r.at[0, p], ref)
        half = part_of(below, p, 0)
        rcopy(half, half, t3f_s, t3_r.at[2, p], fs, above).start()
        to_core(below, p)
        ref = part_of(above, p)
        wait_for(t3_r.at[1, p], ref)
        half = part_of(above, p, 1)
        rcopy(half, half, t3f_s, t3_r.at[2, p], fs, below).start()
        to_core(above, p)
    for p in range(NX):
        wait_for(t3_r.at[2, p], part_of(tp_of(2), p))
        to_core(tp_of(2), p)
    wait_for(cc_r, xg.at[0:NY])
    wait_for(gu_r, wgu.at[0 : (NFS - 1) * 128, :])

    outs = [
        pltpu.make_async_copy(wgu.at[:, 0:128], gate_out, out_sem.at[0]),
        pltpu.make_async_copy(wgu.at[:, 128:256], up_out, out_sem.at[1]),
    ]
    for cp in outs:
        cp.start()

    my_lanes = pl.ds(pl.multiple_of(tp * 128, 128), 128)

    @pl.loop(0, NX)
    def _(r):
        rows = pl.ds(pl.multiple_of(r * XROWS, XROWS), XROWS)
        acc = jnp.zeros((XROWS, 256), F32)
        for t in range(NTP):
            acc += jnp.dot(
                xg[t, rows, :], wgu[t * KB : (t + 1) * KB, :], preferred_element_type=F32
            )
        g, u = acc[:, 0:128], acc[:, 128:256]
        hid[rows, my_lanes] = (g / (1.0 + jnp.exp(-g)) * u).astype(BF16)

    def lanes_of(t):
        return hid.at[:, pl.ds(pl.multiple_of(t * 128, 128), 128)]

    own_h = lanes_of(tp)
    for dy in (1, 3, 2):
        rcopy(own_h, own_h, h_s, h_r.at[dy - 1], fs, tp_of(dy)).start()
    rcopy(own_h, own_h, hc_s, hc_r, fs, other).start()
    for dy in (1, 3, 2):
        ref = lanes_of(tp_of(NY - dy))
        wait_for(h_r.at[dy - 1], ref)
        rcopy(ref, ref, hc_s, hc_r, fs, other).start()
    wait_for(hc_r, hid.at[:, 0 : NY * 128])

    def summed(k):
        wait_for(r1_r.at[k], r1.at[k])
        total = ro[k, x].astype(F32)
        for i in range(NX - 1):
            total += r1[k, i].astype(F32)
        r2[k] = total.astype(BF16).reshape(NZ, SLOT, CW)
        cols = slice(k * CW, (k + 1) * CW)
        rr[z, :, cols] = r2[k, z]

        @pl.loop(1, NZ)
        def _(dz):
            z2 = rem(z + dz, NZ)
            rcopy(
                r2.at[k, z2], rr.at[z, :, cols], r2_s.at[k], r2_r.at[k], z2 * NX + x, tp
            ).start()

    out_down = []
    for k in range(NC):
        part = slice(k * DR, (k + 1) * DR)
        wait_for(wd_r.at[k], sd.at[0 : NFS - 1, 0:DR, :])
        if k + 2 < NC:

            @pl.loop(1, NFS)
            def _(i):
                send_down(k + 2, i)

        @pl.loop(1, NTP)
        def _(i):
            t2_ = rem(tp + i, NTP)
            rcopy(
                wd.at[t2_, :, part, :], dn.at[k, :, :, my_lanes], dn_s.at[k], dn_r.at[k], fs, t2_
            ).start()

        dn[k, :, :, my_lanes] = wd[tp, :, part, :]
        cp = pltpu.make_async_copy(wd.at[:, :, part, :], down_out.at[:, :, part, :], outd_sem.at[k])
        cp.start()
        out_down.append(cp)
        wait_for(dn_r.at[k], sd.at[0 : 4 * (NTP - 1), 0:DR, :])
        dnk = dn[k].reshape(CW, NTP * 128)
        for j in (1, 2, 3, 0):
            x2 = rem(x + j, NX)
            rows = pl.ds(pl.multiple_of(x2 * XROWS, XROWS), XROWS)
            ro[k, x2] = lax.dot_general(
                hid[rows, :], dnk, (((1,), (1,)), ((), ())), preferred_element_type=F32
            ).astype(BF16)
        for j in (1, 2, 3):
            x2 = rem(x + j, NX)
            rcopy(
                ro.at[k, x2], r1.at[k, j - 1], r1_s.at[k], r1_r.at[k], z * NX + x2, tp
            ).start()
        if k >= 1:
            summed(k - 1)
    summed(NC - 1)

    for k in range(NC):
        wait_for(r2_r.at[k], r2.at[k, 0 : NZ - 1])
    got = rr[...].astype(F32)
    per_expert = jnp.concatenate([got[2 * e] + got[2 * e + 1] for e in range(EXPERTS)], axis=0)
    mixed_ref[...] = jnp.dot(
        wmix[...], per_expert, precision=lax.Precision.HIGHEST, preferred_element_type=F32
    ).astype(BF16)

    wait_for(t1_s, xg.at[0, 0 : (NZ - 1) * SLOT, :])
    for cp in t2:
        cp.wait_send()
    wait_for(t3_s, xg.at[0:2])
    wait_for(t3f_s, xg.at[0])
    wait_for(cc_s, xg.at[0:NY])
    wait_for(gu_s, wgu.at[0 : (NFS - 1) * 128, :])
    wait_for(h_s, hid.at[:, 0 : (NY - 1) * 128])
    wait_for(hc_s, hid.at[:, 0 : NY * 128])
    for k in range(NC):
        wait_for(wd_s.at[k], sd.at[0 : NFS - 1, 0:DR, :])
        wait_for(dn_s.at[k], sd.at[0 : 4 * (NTP - 1), 0:DR, :])
        wait_for(r1_s.at[k], r1.at[k])
        wait_for(r2_s.at[k], r2.at[k, 0 : NZ - 1])
    for cp in outs + out_down:
        cp.wait()


def per_device(tokens, routes, route_logits, norm_gain, gate_weight, up_weight, down_weight):
    dma = pltpu.SemaphoreType.DMA
    hbm = pl.BlockSpec(memory_space=pl.ANY)
    vmem = pl.BlockSpec(memory_space=pltpu.VMEM)
    mixed, gate, up, down = pl.pallas_call(
        kernel,
        out_shape=(
            jax.ShapeDtypeStruct((TOK, KB), BF16),
            jax.ShapeDtypeStruct((D, 128), BF16),
            jax.ShapeDtypeStruct((D, 128), BF16),
            jax.ShapeDtypeStruct((NZ, NX, 128, 128), BF16),
        ),
        in_specs=[hbm, vmem, vmem, vmem, hbm, hbm, hbm],
        out_specs=(vmem, hbm, hbm, hbm),
        scratch_shapes=[
            pltpu.VMEM((TOK, D), BF16),
            pltpu.VMEM((3, EXPERTS, 128, 1024), F32),
            pltpu.VMEM((TOK, EXPERTS * SLOT), F32),
            pltpu.VMEM((EXPERTS, SLOT, KB), BF16),
            pltpu.VMEM((NFS, 128, 256), BF16),
            pltpu.VMEM((NFS, 128, 128), BF16),
            pltpu.VMEM((D, 256), BF16),
            pltpu.VMEM((NZ, NX, 128, 128), BF16),
            pltpu.VMEM((NTP, ROWS, KB), BF16),
            pltpu.VMEM((ROWS, NTP * 128), BF16),
            pltpu.VMEM((NC, NX, DR, NTP * 128), BF16),
            pltpu.VMEM((NC, NX, XROWS, CW), BF16),
            pltpu.VMEM((NC, NX - 1, XROWS, CW), BF16),
            pltpu.VMEM((NC, NZ, SLOT, CW), BF16),
            pltpu.VMEM((NZ, SLOT, KB), BF16),
            dma, dma((3,)),
            dma, dma, dma((NX - 1,)), dma((NX - 1,)), dma, dma((3, NX)), dma, dma, dma,
            dma, dma, dma((NC,)), dma((NC,)), dma, dma((NY - 1,)), dma, dma,
            dma((NC,)), dma((NC,)), dma((NC,)), dma((NC,)), dma((NC,)), dma((NC,)),
            dma((2,)), dma((NC,)),
        ],
        compiler_params=pltpu.CompilerParams(
            collective_id=0, has_side_effects=True, vmem_limit_bytes=56 * 2**20
        ),
        name="expert_handover",
    )(tokens, routes, route_logits, norm_gain[None, :], gate_weight, up_weight, down_weight)
    mixed = mixed.reshape(TOK, NC, NX, DR).transpose(0, 2, 1, 3).reshape(TOK, KB)
    return (mixed, gate[None], up[None], down.reshape(1, D, 128))


def solution(mesh):
    in_specs = (
        P("fs", None),
        P("fs", None),
        P("fs", None),
        P("fs"),
        P(None, "fs", "tp"),
        P(None, "fs", "tp"),
        P(None, "fs", "tp"),
    )
    out_specs = (P("fs", "tp"), P("tp", None, "fs"), P("tp", None, "fs"), P("tp", None, "fs"))
    return jax.shard_map(
        per_device, mesh=mesh, in_specs=in_specs, out_specs=out_specs, check_vma=False
    )
```

```python
import functools

import jax
import jax.numpy as jnp
from jax import lax
from jax.experimental import pallas as pl
from jax.experimental.pallas import tpu as pltpu
from jax.sharding import PartitionSpec as P

MESH = pl.DeviceIdType.MESH
NZ, NX, NY = 8, 4, 4
NFS, NTP = 32, 8
EXPERTS = 4
D = 4096
KB = D // NTP
TOK = 40
SLOT = 32
ROWS = NFS * SLOT
XROWS = NZ * SLOT
NC = 4
DR = 128 // NC
CW = NX * DR
F32, BF16 = jnp.float32, jnp.bfloat16


def rem(a, n):
    return lax.rem(a, jnp.int32(n))


def div(a, n):
    return lax.div(a, jnp.int32(n))


def kernel(
    tok_hbm, routes_hbm, logits_hbm, gain_hbm, gate_hbm, up_hbm, down_hbm,
    mixed_ref, wgu, wd,
    tok, routes_ref, logits_ref, gain_ref, stage, wmix, p_send, sg, sd, xg, hid, dn, ro, r1, r2, rr,
    tok_sem, load_sem,
    t1_s, t1_r, t2_s, t2_r, t3_s, t3_r, t3f_s, cc_s, cc_r,
    gu_s, gu_r, wd_s, wd_r, h_s, h_r, hc_s, hc_r, dn_s, dn_r, r1_s, r1_r, r2_s, r2_r,
):
    fs, tp = lax.axis_index("fs"), lax.axis_index("tp")
    z, x = div(fs, NX), rem(fs, NX)
    y, core = div(tp, 2), rem(tp, 2)

    def rcopy(src, dst, ssem, rsem, fs2, tp2):
        return pltpu.make_async_remote_copy(
            src_ref=src, dst_ref=dst, send_sem=ssem, recv_sem=rsem,
            device_id=(fs2, tp2), device_id_type=MESH,
        )

    def wait_for(sem, ref):
        pltpu.make_async_copy(ref, ref, sem).wait()

    def tp_of(dy):
        return rem(y + dy, NY) * 2 + core

    other = y * 2 + (1 - core)

    small = [
        pltpu.make_async_copy(src, dst, tok_sem.at[i])
        for i, (src, dst) in enumerate(
            ((routes_hbm, routes_ref), (logits_hbm, logits_ref), (tok_hbm, tok), (gain_hbm, gain_ref))
        )
    ]
    for cp in small:
        cp.start()
    loads = []
    for m, hbm in enumerate((gate_hbm, up_hbm, down_hbm)):
        cp = pltpu.make_async_copy(hbm, stage.at[m], load_sem.at[m])
        cp.start()
        loads.append(cp)

    bar = pltpu.get_barrier_semaphore()

    @pl.loop(1, NFS)
    def _(i):
        pl.semaphore_signal(bar, inc=1, device_id=(rem(fs + i, NFS), tp), device_id_type=MESH)

    @pl.loop(1, NTP)
    def _(i):
        pl.semaphore_signal(bar, inc=1, device_id=(fs, rem(tp + i, NTP)), device_id_type=MESH)

    small[0].wait()
    small[1].wait()
    row = lax.broadcasted_iota(jnp.int32, (EXPERTS * SLOT, TOK), 0)
    row_e = div(row, SLOT)
    row_s = rem(row, SLOT).astype(F32)
    pick0 = jnp.where(routes_ref[0:1, :] == row_e, 1.0, 0.0).astype(F32)
    pick1 = jnp.where(routes_ref[1:2, :] == row_e, 1.0, 0.0).astype(F32)
    member = pick0 + pick1
    row_i = lax.broadcasted_iota(jnp.int32, (TOK, TOK), 0)
    col_i = lax.broadcasted_iota(jnp.int32, (TOK, TOK), 1)
    before = jnp.where(row_i < col_i, 1.0, 0.0).astype(BF16)
    position = jnp.dot(member.astype(BF16), before, preferred_element_type=F32)
    placing = jnp.where((position == row_s) & (member > 0.0), 1.0, 0.0).astype(F32)
    diff = logits_ref[0:1, :] - logits_ref[1:2, :]
    share0 = 1.0 / (1.0 + jnp.exp(-diff))
    share1 = 1.0 / (1.0 + jnp.exp(diff))
    wmix[...] = placing * (pick0 * share0 + pick1 * share1)

    small[2].wait()
    tf = tok[...].astype(F32)
    inv = lax.rsqrt(jnp.mean(tf * tf, axis=1, keepdims=True) + 1e-05)
    block = tok[:, pl.ds(pl.multiple_of(tp * KB, KB), KB)].astype(F32)
    normed = (block * inv).astype(BF16)
    packed = jnp.dot(placing.astype(BF16), normed, preferred_element_type=F32)
    p_send[...] = packed.astype(BF16).reshape(EXPERTS, SLOT, KB)
    own_x = pl.multiple_of(x * XROWS, XROWS)
    own_row = pl.multiple_of(x * XROWS + z * SLOT, SLOT)
    xg[tp, pl.ds(own_row, SLOT), :] = p_send[div(z, 2)]

    pl.semaphore_wait(bar, NFS - 1 + NTP - 1)

    for dz in (4, 3, 5, 2, 6, 1, 7):
        z2 = rem(z + dz, NZ)
        rcopy(
            p_send.at[div(z2, 2)], xg.at[tp, pl.ds(own_row, SLOT), :], t1_s, t1_r.at[dz],
            z2 * NX + x, tp,
        ).start()

    my_rows = pl.ds(pl.multiple_of(fs * 128, 128), 128)

    def send_gu(dz, dx):
        f2 = rem(z + dz, NZ) * NX + rem(x + dx, NX)
        rcopy(sg.at[f2], wgu.at[my_rows, :], gu_s, gu_r, f2, tp).start()

    def send_down(k, i):
        dx, dz = div(i, NZ), rem(i, NZ)
        f2 = rem(z + dz, NZ) * NX + rem(x + dx, NX)
        part = pl.ds(k * DR, DR)
        rcopy(
            sd.at[f2, part, :], wd.at[z, x, part, :], wd_s.at[k], wd_r.at[k], f2, tp
        ).start()

    small[3].wait()
    gain = jnp.transpose(jnp.broadcast_to(gain_ref[...], (128, 128)))
    for m in range(2):
        loads[m].wait()

        @pl.loop(0, EXPERTS)
        def _(e):
            for s in range(8):
                sg[e * 8 + s, :, m * 128 : (m + 1) * 128] = (
                    stage[m, e, :, s * 128 : (s + 1) * 128] * gain
                ).astype(BF16)

    wgu[pl.ds(pl.multiple_of(fs * 128, 128), 128), :] = sg[fs]

    @pl.loop(1, NZ)
    def _(dz):
        send_gu(dz, 0)

    loads[2].wait()

    @pl.loop(0, EXPERTS)
    def _(e):
        for s in range(8):
            sd[e * 8 + s] = stage[2, e, :, s * 128 : (s + 1) * 128].astype(BF16)

    wd[z, x] = sd[fs]

    def along_x(dz):
        piece = xg.at[tp, pl.ds(own_x + rem(z + NZ - dz, NZ) * SLOT, SLOT), :]
        if dz:
            wait_for(t1_r.at[dz], piece)
        for dx in (1, 3, 2):
            rcopy(
                piece, piece, t2_s, t2_r.at[dx - 1], z * NX + rem(x + dx, NX), tp
            ).start()

    for dz in (0, 1, 7, 2, 6, 3, 5, 4):
        along_x(dz)

    def part_of(t, p, half=None):
        base = rem(x + NX - p, NX) * XROWS
        if half is None:
            return xg.at[t, pl.ds(pl.multiple_of(base, XROWS), XROWS), :]
        h = XROWS // 2
        return xg.at[t, pl.ds(pl.multiple_of(base + half * h, h), h), :]

    def to_core(t, p):
        ref = part_of(t, p)
        rcopy(ref, ref, cc_s, cc_r, fs, other).start()

    def own_part(p):
        ref = part_of(tp, p)
        rcopy(ref, ref, t3_s, t3_r.at[0, p], fs, tp_of(1)).start()
        rcopy(ref, ref, t3_s, t3_r.at[1, p], fs, tp_of(3)).start()
        to_core(tp, p)

    own_part(0)

    def send_gu_from(dx):
        @pl.loop(0, NZ)
        def _(dz):
            send_gu(dz, dx)

    for p in range(1, NX):
        wait_for(t2_r.at[p - 1], part_of(tp, p))
        own_part(p)
        send_gu_from(p)
    for k in range(NC):

        @pl.loop(1, NFS)
        def _(i):
            send_down(k, i)

    for p in range(NX):
        below, above = tp_of(3), tp_of(1)
        ref = part_of(below, p)
        wait_for(t3_r.at[0, p], ref)
        half = part_of(below, p, 0)
        rcopy(half, half, t3f_s, t3_r.at[2, p], fs, above).start()
        to_core(below, p)
        ref = part_of(above, p)
        wait_for(t3_r.at[1, p], ref)
        half = part_of(above, p, 1)
        rcopy(half, half, t3f_s, t3_r.at[2, p], fs, below).start()
        to_core(above, p)
    for p in range(NX):
        wait_for(t3_r.at[2, p], part_of(tp_of(2), p))
        to_core(tp_of(2), p)
    wait_for(cc_r, xg.at[0:NY])
    wait_for(gu_r, wgu.at[0 : (NFS - 1) * 128, :])


    @pl.loop(0, NX)
    def _(r):
        rows = pl.ds(pl.multiple_of(r * XROWS, XROWS), XROWS)
        acc = jnp.zeros((XROWS, 256), F32)
        for t in range(NTP):
            acc += jnp.dot(
                xg[t, rows, :], wgu[t * KB : (t + 1) * KB, :], preferred_element_type=F32
            )
        g, u = acc[:, 0:128], acc[:, 128:256]
        hid[tp, rows, :] = (g / (1.0 + jnp.exp(-g)) * u).astype(BF16)

    def lanes_of(t):
        return hid.at[t]

    half = ROWS // 2

    def piece_of(t, h):
        return hid.at[t, h * half : (h + 1) * half, :]

    below, above = tp_of(3), tp_of(1)
    for h in (0, 1):
        up_piece, down_piece = piece_of(tp, h), piece_of(tp, 1 - h)
        rcopy(up_piece, up_piece, h_s, h_r.at[0, h], fs, above).start()
        rcopy(down_piece, down_piece, h_s, h_r.at[1, 1 - h], fs, below).start()
    own_h = lanes_of(tp)
    rcopy(own_h, own_h, hc_s, hc_r, fs, other).start()

    def h_core(t):
        rcopy(lanes_of(t), lanes_of(t), hc_s, hc_r, fs, other).start()

    def summed(k):
        wait_for(r1_r.at[k], r1.at[k])
        total = ro[k, x].astype(F32)
        for i in range(NX - 1):
            total += r1[k, i].astype(F32)
        r2[k] = total.astype(BF16).reshape(NZ, SLOT, CW)
        rr[k, z] = r2[k, z]

        @pl.loop(1, NZ)
        def _(dz):
            z2 = rem(z + dz, NZ)
            rcopy(
                r2.at[k, z2], rr.at[k, z], r2_s.at[k], r2_r.at[k], z2 * NX + x, tp
            ).start()

    def forward(k):
        part = slice(k * DR, (k + 1) * DR)
        wait_for(wd_r.at[k], sd.at[0 : NFS - 1, 0:DR, :])

        @pl.loop(1, NTP)
        def _(i):
            to = rem(tp + i, NTP)
            rcopy(
                wd.at[to, :, part, :], dn.at[k, tp], dn_s.at[k], dn_r.at[k], fs, to
            ).start()

        dn[k, tp] = wd[tp, :, part, :]

    def project(k):
        wait_for(dn_r.at[k], sd.at[0 : 4 * (NTP - 1), 0:DR, :])
        dnk = jnp.concatenate([dn[k, t].reshape(CW, 128) for t in range(NTP)], axis=1)
        for j in (1, 2, 3, 0):
            x2 = rem(x + j, NX)
            rows = pl.ds(pl.multiple_of(x2 * XROWS, XROWS), XROWS)
            ro[k, x2] = lax.dot_general(
                jnp.concatenate([hid[t, rows, :] for t in range(NTP)], axis=1),
                dnk, (((1,), (1,)), ((), ())), preferred_element_type=F32
            ).astype(BF16)
        for j in (1, 2, 3):
            x2 = rem(x + j, NX)
            rcopy(
                ro.at[k, x2], r1.at[k, j - 1], r1_s.at[k], r1_r.at[k], z * NX + x2, tp
            ).start()

    forward(0)
    wait_for(h_r.at[0, 0], piece_of(below, 0))
    rcopy(piece_of(below, 0), piece_of(below, 0), h_s, h_r.at[2, 0], fs, above).start()
    wait_for(h_r.at[1, 1], piece_of(above, 1))
    rcopy(piece_of(above, 1), piece_of(above, 1), h_s, h_r.at[2, 0], fs, below).start()
    wait_for(h_r.at[0, 1], piece_of(below, 1))
    h_core(below)
    wait_for(h_r.at[1, 0], piece_of(above, 0))
    h_core(above)
    forward(1)
    wait_for(h_r.at[2, 0], lanes_of(tp_of(2)))
    h_core(tp_of(2))
    forward(2)
    wait_for(hc_r, hid.at[0:NY])
    project(0)
    project(1)
    forward(3)
    project(2)
    summed(0)
    summed(1)
    project(3)
    summed(2)
    summed(3)

    for k in range(NC):
        wait_for(r2_r.at[k], r2.at[k, 0 : NZ - 1])
    per_expert = jnp.concatenate(
        [
            jnp.concatenate(
                [
                    rr[k, 2 * e].astype(F32) + rr[k, 2 * e + 1].astype(F32)
                    for e in range(EXPERTS)
                ],
                axis=0,
            )
            for k in range(NC)
        ],
        axis=1,
    )
    mixed = lax.dot_general(
        wmix[...], per_expert, (((0,), (0,)), ((), ())),
        precision=lax.Precision.HIGHEST, preferred_element_type=F32,
    )
    mixed_ref[...] = jnp.concatenate(
        [
            mixed[:, k * CW + i * DR : k * CW + (i + 1) * DR]
            for i in range(NX)
            for k in range(NC)
        ],
        axis=1,
    ).astype(BF16)

    wait_for(t1_s, xg.at[0, 0 : (NZ - 1) * SLOT, :])
    wait_for(t2_s, xg.at[0, 0 : (NX - 1) * XROWS, :])
    wait_for(t3_s, xg.at[0:2])
    wait_for(t3f_s, xg.at[0])
    wait_for(cc_s, xg.at[0:NY])
    wait_for(gu_s, wgu.at[0 : (NFS - 1) * 128, :])
    wait_for(h_s, hid.at[0 : NY - 1])
    wait_for(hc_s, hid.at[0:NY])
    for k in range(NC):
        wait_for(wd_s.at[k], sd.at[0 : NFS - 1, 0:DR, :])
        wait_for(dn_s.at[k], sd.at[0 : 4 * (NTP - 1), 0:DR, :])
        wait_for(r1_s.at[k], r1.at[k])
        wait_for(r2_s.at[k], r2.at[k, 0 : NZ - 1])


def write_out(mixed_ref, wgu, wd, gate_out, up_out, down_out, mixed_out, sem):
    copies = [
        pltpu.make_async_copy(wgu.at[:, 0:128], gate_out, sem.at[0]),
        pltpu.make_async_copy(wgu.at[:, 128:256], up_out, sem.at[1]),
        pltpu.make_async_copy(wd, down_out, sem.at[2]),
        pltpu.make_async_copy(mixed_ref, mixed_out, sem.at[3]),
    ]
    for cp in copies:
        cp.start()
    for cp in copies:
        cp.wait()


def per_device(tokens, routes, route_logits, norm_gain, gate_weight, up_weight, down_weight):
    dma = pltpu.SemaphoreType.DMA
    hbm = pl.BlockSpec(memory_space=pltpu.HBM)
    vmem = pl.BlockSpec(memory_space=pltpu.VMEM)
    mixed, wgu, wd = pl.pallas_call(
        kernel,
        out_shape=(
            pltpu.VMEM((TOK, KB), BF16),
            pltpu.VMEM((D, 256), BF16),
            pltpu.VMEM((NZ, NX, 128, 128), BF16),
        ),
        in_specs=[hbm] * 7,
        out_specs=(vmem, vmem, vmem),
        scratch_shapes=[
            pltpu.VMEM((TOK, D), BF16),
            pltpu.VMEM((2, TOK), jnp.int32),
            pltpu.VMEM((2, TOK), F32),
            pltpu.VMEM((1, 128), F32),
            pltpu.VMEM((3, EXPERTS, 128, 1024), F32),
            pltpu.VMEM((EXPERTS * SLOT, TOK), F32),
            pltpu.VMEM((EXPERTS, SLOT, KB), BF16),
            pltpu.VMEM((NFS, 128, 256), BF16),
            pltpu.VMEM((NFS, 128, 128), BF16),
            pltpu.VMEM((NTP, ROWS, KB), BF16),
            pltpu.VMEM((NTP, ROWS, 128), BF16),
            pltpu.VMEM((NC, NTP, NX, DR, 128), BF16),
            pltpu.VMEM((NC, NX, XROWS, CW), BF16),
            pltpu.VMEM((NC, NX - 1, XROWS, CW), BF16),
            pltpu.VMEM((NC, NZ, SLOT, CW), BF16),
            pltpu.VMEM((NC, NZ, SLOT, CW), BF16),
            dma((4,)), dma((3,)),
            dma, dma((NZ,)), dma, dma((NX - 1,)), dma, dma((3, NX)), dma, dma, dma,
            dma, dma, dma((NC,)), dma((NC,)), dma, dma((3, 2)), dma, dma,
            dma((NC,)), dma((NC,)), dma((NC,)), dma((NC,)), dma((NC,)), dma((NC,)),
        ],
        compiler_params=pltpu.CompilerParams(
            collective_id=0, has_side_effects=True, vmem_limit_bytes=48 * 2**20
        ),
        name="expert_handover",
    )(
        *(
            pltpu.with_memory_space_constraint(a, pltpu.HBM)
            for a in (
                tokens, routes.T, route_logits.T, norm_gain[None, :],
                gate_weight, up_weight, down_weight,
            )
        )
    )
    gate, up, down, mixed = pl.pallas_call(
        write_out,
        out_shape=(
            jax.ShapeDtypeStruct((D, 128), BF16),
            jax.ShapeDtypeStruct((D, 128), BF16),
            jax.ShapeDtypeStruct((NZ, NX, 128, 128), BF16),
            jax.ShapeDtypeStruct((TOK, KB), BF16),
        ),
        in_specs=[vmem, vmem, vmem],
        out_specs=(hbm, hbm, hbm, hbm),
        scratch_shapes=[dma((4,))],
        compiler_params=pltpu.CompilerParams(vmem_limit_bytes=2**20),
        name="write_out",
    )(*(pltpu.with_memory_space_constraint(a, pltpu.VMEM) for a in (mixed, wgu, wd)))
    return (mixed, gate[None], up[None], down.reshape(1, D, 128))


def solution(mesh):
    in_specs = (
        P("fs", None),
        P("fs", None),
        P("fs", None),
        P("fs"),
        P(None, "fs", "tp"),
        P(None, "fs", "tp"),
        P(None, "fs", "tp"),
    )
    out_specs = (P("fs", "tp"), P("tp", None, "fs"), P("tp", None, "fs"), P("tp", None, "fs"))
    return jax.shard_map(
        per_device, mesh=mesh, in_specs=in_specs, out_specs=out_specs, check_vma=False
    )
```

```python
import functools

import jax
import jax.numpy as jnp
from jax import lax
from jax.experimental import pallas as pl
from jax.experimental.pallas import tpu as pltpu
from jax.sharding import PartitionSpec as P

MESH = pl.DeviceIdType.MESH
NZ, NX, NY = 8, 4, 4
NFS, NTP = 32, 8
EXPERTS = 4
D = 4096
KB = D // NTP
TOK = 40
SLOT = 32
ROWS = NFS * SLOT
XROWS = NZ * SLOT
NC = 4
DR = 128 // NC
CW = NX * DR
F32, BF16 = jnp.float32, jnp.bfloat16


def rem(a, n):
    return lax.rem(a, jnp.int32(n))


def div(a, n):
    return lax.div(a, jnp.int32(n))


def kernel(
    tok_hbm, routes_hbm, logits_hbm, gain_hbm, gate_hbm, up_hbm, down_hbm,
    mixed_ref, wgu, wd,
    tok, routes_ref, logits_ref, gain_ref, stage, wmix, p_send, sg, sd, xg, hid, dn, ro, r1, r2, rr,
    tok_sem, load_sem,
    t1_s, t1_r, t2_s, t2_r, t3_s, t3_r, t3f_s, cc_s, cc_r,
    go, gu_s, gu_r, wd_s, wd_r, h_s, h_r, hc_s, hc_r, dn_s, dn_r, r1_s, r1_r, r2_s, r2_r,
):
    fs, tp = lax.axis_index("fs"), lax.axis_index("tp")
    z, x = div(fs, NX), rem(fs, NX)
    y, core = div(tp, 2), rem(tp, 2)

    def rcopy(src, dst, ssem, rsem, fs2, tp2):
        return pltpu.make_async_remote_copy(
            src_ref=src, dst_ref=dst, send_sem=ssem, recv_sem=rsem,
            device_id=(fs2, tp2), device_id_type=MESH,
        )

    def wait_for(sem, ref):
        pltpu.make_async_copy(ref, ref, sem).wait()

    def tp_of(dy):
        return rem(y + dy, NY) * 2 + core

    other = y * 2 + (1 - core)

    small = [
        pltpu.make_async_copy(src, dst, tok_sem.at[i])
        for i, (src, dst) in enumerate(
            ((routes_hbm, routes_ref), (logits_hbm, logits_ref), (tok_hbm, tok), (gain_hbm, gain_ref))
        )
    ]
    for cp in small:
        cp.start()
    loads = []
    for m, hbm in enumerate((gate_hbm, up_hbm, down_hbm)):
        cp = pltpu.make_async_copy(hbm, stage.at[m], load_sem.at[m])
        cp.start()
        loads.append(cp)

    bar = pltpu.get_barrier_semaphore()

    @pl.loop(1, NFS)
    def _(i):
        pl.semaphore_signal(bar, inc=1, device_id=(rem(fs + i, NFS), tp), device_id_type=MESH)

    @pl.loop(1, NTP)
    def _(i):
        pl.semaphore_signal(bar, inc=1, device_id=(fs, rem(tp + i, NTP)), device_id_type=MESH)

    small[0].wait()
    small[1].wait()
    row = lax.broadcasted_iota(jnp.int32, (EXPERTS * SLOT, TOK), 0)
    row_e = div(row, SLOT)
    row_s = rem(row, SLOT).astype(F32)
    pick0 = jnp.where(routes_ref[0:1, :] == row_e, 1.0, 0.0).astype(F32)
    pick1 = jnp.where(routes_ref[1:2, :] == row_e, 1.0, 0.0).astype(F32)
    member = pick0 + pick1
    row_i = lax.broadcasted_iota(jnp.int32, (TOK, TOK), 0)
    col_i = lax.broadcasted_iota(jnp.int32, (TOK, TOK), 1)
    before = jnp.where(row_i < col_i, 1.0, 0.0).astype(BF16)
    position = jnp.dot(member.astype(BF16), before, preferred_element_type=F32)
    placing = jnp.where((position == row_s) & (member > 0.0), 1.0, 0.0).astype(F32)
    diff = logits_ref[0:1, :] - logits_ref[1:2, :]
    share0 = 1.0 / (1.0 + jnp.exp(-diff))
    share1 = 1.0 / (1.0 + jnp.exp(diff))
    wmix[...] = placing * (pick0 * share0 + pick1 * share1)

    small[2].wait()
    tf = tok[...].astype(F32)
    inv = lax.rsqrt(jnp.mean(tf * tf, axis=1, keepdims=True) + 1e-05)
    block = tok[:, pl.ds(pl.multiple_of(tp * KB, KB), KB)].astype(F32)
    normed = (block * inv).astype(BF16)
    packed = jnp.dot(placing.astype(BF16), normed, preferred_element_type=F32)
    p_send[...] = packed.astype(BF16).reshape(EXPERTS, SLOT, KB)
    own_x = pl.multiple_of(x * XROWS, XROWS)
    own_row = pl.multiple_of(x * XROWS + z * SLOT, SLOT)
    xg[tp, pl.ds(own_row, SLOT), :] = p_send[div(z, 2)]

    pl.semaphore_wait(bar, NFS - 1 + NTP - 1)

    for dz in (4, 3, 5, 2, 6, 1, 7):
        z2 = rem(z + dz, NZ)
        rcopy(
            p_send.at[div(z2, 2)], xg.at[tp, pl.ds(own_row, SLOT), :], t1_s, t1_r.at[dz],
            z2 * NX + x, tp,
        ).start()

    my_rows = pl.ds(pl.multiple_of(fs * 128, 128), 128)

    def send_gu(dz, dx):
        f2 = rem(z + dz, NZ) * NX + rem(x + dx, NX)
        rcopy(sg.at[f2], wgu.at[my_rows, :], gu_s, gu_r, f2, tp).start()

    def send_down(k, i):
        dx, dz = div(i, NZ), rem(i, NZ)
        f2 = rem(z + dz, NZ) * NX + rem(x + dx, NX)
        part = pl.ds(k * DR, DR)
        rcopy(
            sd.at[f2, part, :], wd.at[z, x, part, :], wd_s.at[k], wd_r.at[k], f2, tp
        ).start()

    small[3].wait()
    gain = jnp.transpose(jnp.broadcast_to(gain_ref[...], (128, 128)))
    for m in range(2):
        loads[m].wait()

        @pl.loop(0, EXPERTS)
        def _(e):
            for s in range(8):
                sg[e * 8 + s, :, m * 128 : (m + 1) * 128] = (
                    stage[m, e, :, s * 128 : (s + 1) * 128] * gain
                ).astype(BF16)

    wgu[pl.ds(pl.multiple_of(fs * 128, 128), 128), :] = sg[fs]

    @pl.loop(1, NZ)
    def _(dz):
        send_gu(dz, 0)

    loads[2].wait()

    @pl.loop(0, EXPERTS)
    def _(e):
        for s in range(8):
            sd[e * 8 + s] = stage[2, e, :, s * 128 : (s + 1) * 128].astype(BF16)

    wd[z, x] = sd[fs]

    def along_x(dz):
        piece = xg.at[tp, pl.ds(own_x + rem(z + NZ - dz, NZ) * SLOT, SLOT), :]
        if dz:
            wait_for(t1_r.at[dz], piece)
        for dx in (1, 3, 2):
            rcopy(
                piece, piece, t2_s, t2_r.at[dx - 1], z * NX + rem(x + dx, NX), tp
            ).start()

    for dz in (0, 1, 7, 2, 6, 3, 5, 4):
        along_x(dz)

    def part_of(t, p, half=None):
        base = rem(x + NX - p, NX) * XROWS
        if half is None:
            return xg.at[t, pl.ds(pl.multiple_of(base, XROWS), XROWS), :]
        h = XROWS // 2
        return xg.at[t, pl.ds(pl.multiple_of(base + half * h, h), h), :]

    def to_core(t, p):
        ref = part_of(t, p)
        rcopy(ref, ref, cc_s, cc_r, fs, other).start()

    def own_part(p):
        ref = part_of(tp, p)
        rcopy(ref, ref, t3_s, t3_r.at[0, p], fs, tp_of(1)).start()
        rcopy(ref, ref, t3_s, t3_r.at[1, p], fs, tp_of(3)).start()
        to_core(tp, p)

    own_part(0)

    def send_gu_from(dx):
        @pl.loop(0, NZ)
        def _(dz):
            send_gu(dz, dx)

    for p in range(1, NX):
        wait_for(t2_r.at[p - 1], part_of(tp, p))
        own_part(p)
        send_gu_from(p)
    def send_all_down():
        for k in range(NC):

            @pl.loop(1, NFS)
            def _(i):
                send_down(k, i)

    @pl.when(core == 0)
    def _():
        send_all_down()

    for p in range(NX):
        below, above = tp_of(3), tp_of(1)
        ref = part_of(below, p)
        wait_for(t3_r.at[0, p], ref)
        half = part_of(below, p, 0)
        rcopy(half, half, t3f_s, t3_r.at[2, p], fs, above).start()
        to_core(below, p)
        ref = part_of(above, p)
        wait_for(t3_r.at[1, p], ref)
        half = part_of(above, p, 1)
        rcopy(half, half, t3f_s, t3_r.at[2, p], fs, below).start()
        to_core(above, p)
    for p in range(NX):
        wait_for(t3_r.at[2, p], part_of(tp_of(2), p))
        to_core(tp_of(2), p)
    wait_for(cc_r, xg.at[0:NY])

    @pl.when(core == 0)
    def _():
        wait_for(gu_s, wgu.at[0 : (NFS - 1) * 128, :])
        pl.semaphore_signal(go, inc=1, device_id=(fs, other), device_id_type=MESH)

    wait_for(gu_r, wgu.at[0 : (NFS - 1) * 128, :])


    @pl.loop(0, NX)
    def _(r):
        rows = pl.ds(pl.multiple_of(r * XROWS, XROWS), XROWS)
        acc = jnp.zeros((XROWS, 256), F32)
        for t in range(NTP):
            acc += jnp.dot(
                xg[t, rows, :], wgu[t * KB : (t + 1) * KB, :], preferred_element_type=F32
            )
        g, u = acc[:, 0:128], acc[:, 128:256]
        hid[tp, rows, :] = (g / (1.0 + jnp.exp(-g)) * u).astype(BF16)

    def lanes_of(t):
        return hid.at[t]

    half = ROWS // 2

    def piece_of(t, h):
        return hid.at[t, h * half : (h + 1) * half, :]

    below, above = tp_of(3), tp_of(1)
    for h in (0, 1):
        up_piece, down_piece = piece_of(tp, h), piece_of(tp, 1 - h)
        rcopy(up_piece, up_piece, h_s, h_r.at[0, h], fs, above).start()
        rcopy(down_piece, down_piece, h_s, h_r.at[1, 1 - h], fs, below).start()
    own_h = lanes_of(tp)
    rcopy(own_h, own_h, hc_s, hc_r, fs, other).start()

    def h_core(t):
        rcopy(lanes_of(t), lanes_of(t), hc_s, hc_r, fs, other).start()

    def summed(k):
        wait_for(r1_r.at[k], r1.at[k])
        total = ro[k, x].astype(F32)
        for i in range(NX - 1):
            total += r1[k, i].astype(F32)
        r2[k] = total.astype(BF16).reshape(NZ, SLOT, CW)
        rr[k, z] = r2[k, z]

        @pl.loop(1, NZ)
        def _(dz):
            z2 = rem(z + dz, NZ)
            rcopy(
                r2.at[k, z2], rr.at[k, z], r2_s.at[k], r2_r.at[k], z2 * NX + x, tp
            ).start()

    def forward(k):
        part = slice(k * DR, (k + 1) * DR)
        wait_for(wd_r.at[k], sd.at[0 : NFS - 1, 0:DR, :])

        @pl.loop(1, NTP)
        def _(i):
            to = rem(tp + i, NTP)
            rcopy(
                wd.at[to, :, part, :], dn.at[k, tp], dn_s.at[k], dn_r.at[k], fs, to
            ).start()

        dn[k, tp] = wd[tp, :, part, :]

    def project(k):
        wait_for(dn_r.at[k], sd.at[0 : 4 * (NTP - 1), 0:DR, :])
        dnk = jnp.concatenate([dn[k, t].reshape(CW, 128) for t in range(NTP)], axis=1)
        for j in (1, 2, 3, 0):
            x2 = rem(x + j, NX)
            rows = pl.ds(pl.multiple_of(x2 * XROWS, XROWS), XROWS)
            ro[k, x2] = lax.dot_general(
                jnp.concatenate([hid[t, rows, :] for t in range(NTP)], axis=1),
                dnk, (((1,), (1,)), ((), ())), preferred_element_type=F32
            ).astype(BF16)
        for j in (1, 2, 3):
            x2 = rem(x + j, NX)
            rcopy(
                ro.at[k, x2], r1.at[k, j - 1], r1_s.at[k], r1_r.at[k], z * NX + x2, tp
            ).start()

    @pl.when(core == 1)
    def _():
        pl.semaphore_wait(go, 1)
        send_all_down()
        wait_for(gu_s, wgu.at[0 : (NFS - 1) * 128, :])

    def relay_near():
        wait_for(h_r.at[0, 0], piece_of(below, 0))
        rcopy(piece_of(below, 0), piece_of(below, 0), h_s, h_r.at[2, 0], fs, above).start()
        wait_for(h_r.at[1, 1], piece_of(above, 1))
        rcopy(piece_of(above, 1), piece_of(above, 1), h_s, h_r.at[2, 0], fs, below).start()
        wait_for(h_r.at[0, 1], piece_of(below, 1))
        h_core(below)
        wait_for(h_r.at[1, 0], piece_of(above, 0))
        h_core(above)

    def relay_far():
        wait_for(h_r.at[2, 0], lanes_of(tp_of(2)))
        h_core(tp_of(2))

    @pl.when(core == 0)
    def _():
        forward(0)
        relay_near()
        forward(1)
        relay_far()

    @pl.when(core == 1)
    def _():
        relay_near()
        relay_far()
        forward(0)
        forward(1)

    forward(2)
    wait_for(hc_r, hid.at[0:NY])
    project(0)
    project(1)
    forward(3)
    project(2)
    summed(0)
    summed(1)
    project(3)
    summed(2)
    summed(3)

    for k in range(NC):
        wait_for(r2_r.at[k], r2.at[k, 0 : NZ - 1])
    per_expert = jnp.concatenate(
        [
            jnp.concatenate(
                [
                    rr[k, 2 * e].astype(F32) + rr[k, 2 * e + 1].astype(F32)
                    for e in range(EXPERTS)
                ],
                axis=0,
            )
            for k in range(NC)
        ],
        axis=1,
    )
    mixed = lax.dot_general(
        wmix[...], per_expert, (((0,), (0,)), ((), ())),
        precision=lax.Precision.HIGHEST, preferred_element_type=F32,
    )
    mixed_ref[...] = jnp.concatenate(
        [
            mixed[:, k * CW + i * DR : k * CW + (i + 1) * DR]
            for i in range(NX)
            for k in range(NC)
        ],
        axis=1,
    ).astype(BF16)

    wait_for(t1_s, xg.at[0, 0 : (NZ - 1) * SLOT, :])
    wait_for(t2_s, xg.at[0, 0 : (NX - 1) * XROWS, :])
    wait_for(t3_s, xg.at[0:2])
    wait_for(t3f_s, xg.at[0])
    wait_for(cc_s, xg.at[0:NY])
    wait_for(h_s, hid.at[0 : NY - 1])
    wait_for(hc_s, hid.at[0:NY])
    for k in range(NC):
        wait_for(wd_s.at[k], sd.at[0 : NFS - 1, 0:DR, :])
        wait_for(dn_s.at[k], sd.at[0 : 4 * (NTP - 1), 0:DR, :])
        wait_for(r1_s.at[k], r1.at[k])
        wait_for(r2_s.at[k], r2.at[k, 0 : NZ - 1])


def write_out(mixed_ref, wgu, wd, gate_out, up_out, down_out, mixed_out, sem):
    copies = [
        pltpu.make_async_copy(wgu.at[:, 0:128], gate_out, sem.at[0]),
        pltpu.make_async_copy(wgu.at[:, 128:256], up_out, sem.at[1]),
        pltpu.make_async_copy(wd, down_out, sem.at[2]),
        pltpu.make_async_copy(mixed_ref, mixed_out, sem.at[3]),
    ]
    for cp in copies:
        cp.start()
    for cp in copies:
        cp.wait()


def per_device(tokens, routes, route_logits, norm_gain, gate_weight, up_weight, down_weight):
    dma = pltpu.SemaphoreType.DMA
    hbm = pl.BlockSpec(memory_space=pltpu.HBM)
    vmem = pl.BlockSpec(memory_space=pltpu.VMEM)
    mixed, wgu, wd = pl.pallas_call(
        kernel,
        out_shape=(
            pltpu.VMEM((TOK, KB), BF16),
            pltpu.VMEM((D, 256), BF16),
            pltpu.VMEM((NZ, NX, 128, 128), BF16),
        ),
        in_specs=[hbm] * 7,
        out_specs=(vmem, vmem, vmem),
        scratch_shapes=[
            pltpu.VMEM((TOK, D), BF16),
            pltpu.VMEM((2, TOK), jnp.int32),
            pltpu.VMEM((2, TOK), F32),
            pltpu.VMEM((1, 128), F32),
            pltpu.VMEM((3, EXPERTS, 128, 1024), F32),
            pltpu.VMEM((EXPERTS * SLOT, TOK), F32),
            pltpu.VMEM((EXPERTS, SLOT, KB), BF16),
            pltpu.VMEM((NFS, 128, 256), BF16),
            pltpu.VMEM((NFS, 128, 128), BF16),
            pltpu.VMEM((NTP, ROWS, KB), BF16),
            pltpu.VMEM((NTP, ROWS, 128), BF16),
            pltpu.VMEM((NC, NTP, NX, DR, 128), BF16),
            pltpu.VMEM((NC, NX, XROWS, CW), BF16),
            pltpu.VMEM((NC, NX - 1, XROWS, CW), BF16),
            pltpu.VMEM((NC, NZ, SLOT, CW), BF16),
            pltpu.VMEM((NC, NZ, SLOT, CW), BF16),
            dma((4,)), dma((3,)),
            dma, dma((NZ,)), dma, dma((NX - 1,)), dma, dma((3, NX)), dma, dma, dma,
            pltpu.SemaphoreType.REGULAR,
            dma, dma, dma((NC,)), dma((NC,)), dma, dma((3, 2)), dma, dma,
            dma((NC,)), dma((NC,)), dma((NC,)), dma((NC,)), dma((NC,)), dma((NC,)),
        ],
        compiler_params=pltpu.CompilerParams(
            collective_id=0, has_side_effects=True, vmem_limit_bytes=48 * 2**20
        ),
        name="expert_handover",
    )(
        *(
            pltpu.with_memory_space_constraint(a, pltpu.HBM)
            for a in (
                tokens, routes.T, route_logits.T, norm_gain[None, :],
                gate_weight, up_weight, down_weight,
            )
        )
    )
    gate, up, down, mixed = pl.pallas_call(
        write_out,
        out_shape=(
            jax.ShapeDtypeStruct((D, 128), BF16),
            jax.ShapeDtypeStruct((D, 128), BF16),
            jax.ShapeDtypeStruct((NZ, NX, 128, 128), BF16),
            jax.ShapeDtypeStruct((TOK, KB), BF16),
        ),
        in_specs=[vmem, vmem, vmem],
        out_specs=(hbm, hbm, hbm, hbm),
        scratch_shapes=[dma((4,))],
        compiler_params=pltpu.CompilerParams(vmem_limit_bytes=2**20),
        name="write_out",
    )(*(pltpu.with_memory_space_constraint(a, pltpu.VMEM) for a in (mixed, wgu, wd)))
    return (mixed, gate[None], up[None], down.reshape(1, D, 128))


def solution(mesh):
    in_specs = (
        P("fs", None),
        P("fs", None),
        P("fs", None),
        P("fs"),
        P(None, "fs", "tp"),
        P(None, "fs", "tp"),
        P(None, "fs", "tp"),
    )
    out_specs = (P("fs", "tp"), P("tp", None, "fs"), P("tp", None, "fs"), P("tp", None, "fs"))
    return jax.shard_map(
        per_device, mesh=mesh, in_specs=in_specs, out_specs=out_specs, check_vma=False
    )
```

```python
import functools

import jax
import jax.numpy as jnp
from jax import lax
from jax.experimental import pallas as pl
from jax.experimental.pallas import tpu as pltpu
from jax.sharding import PartitionSpec as P

MESH = pl.DeviceIdType.MESH
NZ, NX, NY = 8, 4, 4
NFS, NTP = 32, 8
EXPERTS = 4
D = 4096
KB = D // NTP
TOK = 40
SLOT = 32
ROWS = NFS * SLOT
XROWS = NZ * SLOT
CHUNKS = ((0, 32), (32, 32), (64, 32), (96, 16), (112, 16))
NC = len(CHUNKS)
DR = 32
CW = NX * DR
F32, BF16 = jnp.float32, jnp.bfloat16


def rem(a, n):
    return lax.rem(a, jnp.int32(n))


def div(a, n):
    return lax.div(a, jnp.int32(n))


def slots_of(k):
    return SLOT * CHUNKS[k][1] // DR


def kernel(
    tok_hbm, routes_hbm, logits_hbm, gain_hbm, gate_hbm, up_hbm, down_hbm,
    wmix, rr, wgu, wd,
    tok, routes_ref, logits_ref, gain_ref, stage, p_send, sg, sd, xg, hid, dn, ro, r1, r2,
    tok_sem, load_sem,
    t1_s, t1_r, t2_s, t2_r, t3_s, t3_r, t3f_s, cc_s, cc_r,
    go, gu_s, gu_r, wd_s, wd_r, h_s, h_r, hc_s, hc_r, dn_s, dn_r, r1_s, r1_r, r2_s, r2_r,
):
    fs, tp = lax.axis_index("fs"), lax.axis_index("tp")
    z, x = div(fs, NX), rem(fs, NX)
    y, core = div(tp, 2), rem(tp, 2)

    def rcopy(src, dst, ssem, rsem, fs2, tp2):
        return pltpu.make_async_remote_copy(
            src_ref=src, dst_ref=dst, send_sem=ssem, recv_sem=rsem,
            device_id=(fs2, tp2), device_id_type=MESH,
        )

    def wait_for(sem, ref):
        pltpu.make_async_copy(ref, ref, sem).wait()

    def tp_of(dy):
        return rem(y + dy, NY) * 2 + core

    other = y * 2 + (1 - core)

    small = [
        pltpu.make_async_copy(src, dst, tok_sem.at[i])
        for i, (src, dst) in enumerate(
            ((routes_hbm, routes_ref), (logits_hbm, logits_ref), (tok_hbm, tok), (gain_hbm, gain_ref))
        )
    ]
    for cp in small:
        cp.start()
    loads = []
    for m, hbm in enumerate((gate_hbm, up_hbm, down_hbm)):
        cp = pltpu.make_async_copy(hbm, stage.at[m], load_sem.at[m])
        cp.start()
        loads.append(cp)

    bar = pltpu.get_barrier_semaphore()

    @pl.loop(1, NFS)
    def _(i):
        pl.semaphore_signal(bar, inc=1, device_id=(rem(fs + i, NFS), tp), device_id_type=MESH)

    @pl.loop(1, NTP)
    def _(i):
        pl.semaphore_signal(bar, inc=1, device_id=(fs, rem(tp + i, NTP)), device_id_type=MESH)

    small[0].wait()
    small[1].wait()
    row = lax.broadcasted_iota(jnp.int32, (EXPERTS * SLOT, TOK), 0)
    row_e = div(row, SLOT)
    row_s = rem(row, SLOT).astype(F32)
    pick0 = jnp.where(routes_ref[0:1, :] == row_e, 1.0, 0.0).astype(F32)
    pick1 = jnp.where(routes_ref[1:2, :] == row_e, 1.0, 0.0).astype(F32)
    member = pick0 + pick1
    row_i = lax.broadcasted_iota(jnp.int32, (TOK, TOK), 0)
    col_i = lax.broadcasted_iota(jnp.int32, (TOK, TOK), 1)
    before = jnp.where(row_i < col_i, 1.0, 0.0).astype(BF16)
    position = jnp.dot(member.astype(BF16), before, preferred_element_type=F32)
    placing = jnp.where((position == row_s) & (member > 0.0), 1.0, 0.0).astype(F32)
    diff = logits_ref[0:1, :] - logits_ref[1:2, :]
    share0 = 1.0 / (1.0 + jnp.exp(-diff))
    share1 = 1.0 / (1.0 + jnp.exp(diff))
    wmix[...] = placing * (pick0 * share0 + pick1 * share1)

    small[2].wait()
    tf = tok[...].astype(F32)
    inv = lax.rsqrt(jnp.mean(tf * tf, axis=1, keepdims=True) + 1e-05)
    block = tok[:, pl.ds(pl.multiple_of(tp * KB, KB), KB)].astype(F32)
    normed = (block * inv).astype(BF16)
    packed = jnp.dot(placing.astype(BF16), normed, preferred_element_type=F32)
    p_send[...] = packed.astype(BF16).reshape(EXPERTS, SLOT, KB)
    own_x = pl.multiple_of(x * XROWS, XROWS)
    own_row = pl.multiple_of(x * XROWS + z * SLOT, SLOT)
    xg[tp, pl.ds(own_row, SLOT), :] = p_send[div(z, 2)]

    pl.semaphore_wait(bar, NFS - 1 + NTP - 1)

    for dz in (4, 3, 5, 2, 6, 1, 7):
        z2 = rem(z + dz, NZ)
        rcopy(
            p_send.at[div(z2, 2)], xg.at[tp, pl.ds(own_row, SLOT), :], t1_s, t1_r.at[dz],
            z2 * NX + x, tp,
        ).start()

    my_rows = pl.ds(pl.multiple_of(fs * 128, 128), 128)

    def send_gu(dz, dx):
        f2 = rem(z + dz, NZ) * NX + rem(x + dx, NX)
        rcopy(sg.at[f2], wgu.at[my_rows, :], gu_s, gu_r, f2, tp).start()

    def send_down(k, i):
        dx, dz = div(i, NZ), rem(i, NZ)
        f2 = rem(z + dz, NZ) * NX + rem(x + dx, NX)
        part = pl.ds(*CHUNKS[k])
        rcopy(
            sd.at[f2, part, :], wd.at[z, x, part, :], wd_s.at[k], wd_r.at[k], f2, tp
        ).start()

    small[3].wait()
    gain = jnp.transpose(jnp.broadcast_to(gain_ref[...], (128, 128)))
    for m in range(2):
        loads[m].wait()

        @pl.loop(0, EXPERTS)
        def _(e):
            for s in range(8):
                sg[e * 8 + s, :, m * 128 : (m + 1) * 128] = (
                    stage[m, e, :, s * 128 : (s + 1) * 128] * gain
                ).astype(BF16)

    wgu[pl.ds(pl.multiple_of(fs * 128, 128), 128), :] = sg[fs]

    @pl.loop(1, NZ)
    def _(dz):
        send_gu(dz, 0)

    loads[2].wait()

    @pl.loop(0, EXPERTS)
    def _(e):
        for s in range(8):
            sd[e * 8 + s] = stage[2, e, :, s * 128 : (s + 1) * 128].astype(BF16)

    wd[z, x] = sd[fs]

    def along_x(dz):
        piece = xg.at[tp, pl.ds(own_x + rem(z + NZ - dz, NZ) * SLOT, SLOT), :]
        if dz:
            wait_for(t1_r.at[dz], piece)
        for dx in (1, 3, 2):
            rcopy(
                piece, piece, t2_s, t2_r.at[dx - 1], z * NX + rem(x + dx, NX), tp
            ).start()

    for dz in (0, 1, 7, 2, 6, 3, 5, 4):
        along_x(dz)

    def part_of(t, p, half=None):
        base = rem(x + NX - p, NX) * XROWS
        if half is None:
            return xg.at[t, pl.ds(pl.multiple_of(base, XROWS), XROWS), :]
        h = XROWS // 2
        return xg.at[t, pl.ds(pl.multiple_of(base + half * h, h), h), :]

    def to_core(t, p):
        ref = part_of(t, p)
        rcopy(ref, ref, cc_s, cc_r, fs, other).start()

    def own_part(p):
        ref = part_of(tp, p)
        rcopy(ref, ref, t3_s, t3_r.at[0, p], fs, tp_of(1)).start()
        rcopy(ref, ref, t3_s, t3_r.at[1, p], fs, tp_of(3)).start()
        to_core(tp, p)

    own_part(0)

    def send_gu_from(dx):
        @pl.loop(0, NZ)
        def _(dz):
            send_gu(dz, dx)

    for p in range(1, NX):
        wait_for(t2_r.at[p - 1], part_of(tp, p))
        own_part(p)
        send_gu_from(p)
    def send_all_down():
        for k in range(NC):

            @pl.loop(1, NFS)
            def _(i):
                send_down(k, i)

    @pl.when(core == 0)
    def _():
        send_all_down()

    for p in range(NX):
        below, above = tp_of(3), tp_of(1)
        ref = part_of(below, p)
        wait_for(t3_r.at[0, p], ref)
        half = part_of(below, p, 0)
        rcopy(half, half, t3f_s, t3_r.at[2, p], fs, above).start()
        to_core(below, p)
        ref = part_of(above, p)
        wait_for(t3_r.at[1, p], ref)
        half = part_of(above, p, 1)
        rcopy(half, half, t3f_s, t3_r.at[2, p], fs, below).start()
        to_core(above, p)
    for p in range(NX):
        wait_for(t3_r.at[2, p], part_of(tp_of(2), p))
        to_core(tp_of(2), p)
    wait_for(cc_r, xg.at[0:NY])

    @pl.when(core == 0)
    def _():
        wait_for(gu_s, wgu.at[0 : (NFS - 1) * 128, :])
        pl.semaphore_signal(go, inc=1, device_id=(fs, other), device_id_type=MESH)

    wait_for(gu_r, wgu.at[0 : (NFS - 1) * 128, :])


    @pl.loop(0, NX)
    def _(r):
        rows = pl.ds(pl.multiple_of(r * XROWS, XROWS), XROWS)
        acc = jnp.zeros((XROWS, 256), F32)
        for t in range(NTP):
            acc += jnp.dot(
                xg[t, rows, :], wgu[t * KB : (t + 1) * KB, :], preferred_element_type=F32
            )
        g, u = acc[:, 0:128], acc[:, 128:256]
        hid[tp, rows, :] = (g / (1.0 + jnp.exp(-g)) * u).astype(BF16)

    def lanes_of(t):
        return hid.at[t]

    half = ROWS // 2

    def piece_of(t, h):
        return hid.at[t, h * half : (h + 1) * half, :]

    below, above = tp_of(3), tp_of(1)
    for h in (0, 1):
        up_piece, down_piece = piece_of(tp, h), piece_of(tp, 1 - h)
        rcopy(up_piece, up_piece, h_s, h_r.at[0, h], fs, above).start()
        rcopy(down_piece, down_piece, h_s, h_r.at[1, 1 - h], fs, below).start()
    own_h = lanes_of(tp)
    rcopy(own_h, own_h, hc_s, hc_r, fs, other).start()

    def h_core(t):
        rcopy(lanes_of(t), lanes_of(t), hc_s, hc_r, fs, other).start()

    def summed(k):
        n = slots_of(k)
        wait_for(r1_r.at[k], r1.at[k, :, 0 : NZ * n])
        total = ro[k, x, 0 : NZ * n].astype(F32)
        for i in range(NX - 1):
            total += r1[k, i, 0 : NZ * n].astype(F32)
        r2[k, :, 0:n] = total.astype(BF16).reshape(NZ, n, CW)
        rr[k, z, 0:n] = r2[k, z, 0:n]

        @pl.loop(1, NZ)
        def _(dz):
            z2 = rem(z + dz, NZ)
            rcopy(
                r2.at[k, z2, 0:n], rr.at[k, z, 0:n], r2_s.at[k], r2_r.at[k], z2 * NX + x, tp
            ).start()

    def forward(k):
        start, size = CHUNKS[k]
        part = slice(start, start + size)
        wait_for(wd_r.at[k], sd.at[0 : NFS - 1, 0:size, :])

        @pl.loop(1, NTP)
        def _(i):
            to = rem(tp + i, NTP)
            rcopy(
                wd.at[to, :, part, :], dn.at[k, tp, :, 0:size, :], dn_s.at[k], dn_r.at[k], fs, to
            ).start()

        dn[k, tp, :, 0:size, :] = wd[tp, :, part, :]

    def project(k):
        size, n = CHUNKS[k][1], slots_of(k)
        wait_for(dn_r.at[k], sd.at[0 : 4 * (NTP - 1), 0:size, :])
        dnk = jnp.concatenate(
            [dn[k, t, :, 0:size, :].reshape(NX * size, 128) for t in range(NTP)], axis=1
        )
        for j in (1, 2, 3, 0):
            x2 = rem(x + j, NX)
            rows = pl.ds(pl.multiple_of(x2 * XROWS, XROWS), XROWS)
            out = lax.dot_general(
                jnp.concatenate([hid[t, rows, :] for t in range(NTP)], axis=1),
                dnk, (((1,), (1,)), ((), ())), preferred_element_type=F32,
            )
            if n < SLOT:
                out = out.reshape(NZ, 2, n, NX * size)
                out = jnp.concatenate([out[:, 0], out[:, 1]], axis=-1).reshape(NZ * n, CW)
            ro[k, x2, 0 : NZ * n] = out.astype(BF16)
        for j in (1, 2, 3):
            x2 = rem(x + j, NX)
            rcopy(
                ro.at[k, x2, 0 : NZ * n], r1.at[k, j - 1, 0 : NZ * n], r1_s.at[k], r1_r.at[k],
                z * NX + x2, tp,
            ).start()

    @pl.when(core == 1)
    def _():
        pl.semaphore_wait(go, 1)
        send_all_down()
        wait_for(gu_s, wgu.at[0 : (NFS - 1) * 128, :])

    def relay_near():
        wait_for(h_r.at[0, 0], piece_of(below, 0))
        rcopy(piece_of(below, 0), piece_of(below, 0), h_s, h_r.at[2, 0], fs, above).start()
        wait_for(h_r.at[1, 1], piece_of(above, 1))
        rcopy(piece_of(above, 1), piece_of(above, 1), h_s, h_r.at[2, 0], fs, below).start()
        wait_for(h_r.at[0, 1], piece_of(below, 1))
        h_core(below)
        wait_for(h_r.at[1, 0], piece_of(above, 0))
        h_core(above)

    def relay_far():
        wait_for(h_r.at[2, 0], lanes_of(tp_of(2)))
        h_core(tp_of(2))

    @pl.when(core == 0)
    def _():
        forward(0)
        relay_near()
        forward(1)
        relay_far()
        forward(2)

    @pl.when(core == 1)
    def _():
        relay_near()
        relay_far()
        forward(0)
        forward(1)

    wait_for(hc_r, hid.at[0:NY])
    project(0)

    @pl.when(core == 1)
    def _():
        forward(2)

    forward(3)
    project(1)
    forward(4)
    summed(0)
    project(2)
    summed(1)
    project(3)
    project(4)
    summed(2)
    summed(3)
    summed(4)

    for k in range(NC):
        wait_for(r2_r.at[k], r2.at[k, 0 : NZ - 1, 0 : slots_of(k)])

    wait_for(t1_s, xg.at[0, 0 : (NZ - 1) * SLOT, :])
    wait_for(t2_s, xg.at[0, 0 : (NX - 1) * XROWS, :])
    wait_for(t3_s, xg.at[0:2])
    wait_for(t3f_s, xg.at[0])
    wait_for(cc_s, xg.at[0:NY])
    wait_for(h_s, hid.at[0 : NY - 1])
    wait_for(hc_s, hid.at[0:NY])
    for k in range(NC):
        size, n = CHUNKS[k][1], slots_of(k)
        wait_for(wd_s.at[k], sd.at[0 : NFS - 1, 0:size, :])
        wait_for(dn_s.at[k], sd.at[0 : 4 * (NTP - 1), 0:size, :])
        wait_for(r1_s.at[k], r1.at[k, :, 0 : NZ * n])
        wait_for(r2_s.at[k], r2.at[k, 0 : NZ - 1, 0:n])


def write_out(wmix, rr, wgu, wd, gate_out, up_out, down_out, mixed_out, mixed_ref, sem):
    copies = [
        pltpu.make_async_copy(wgu.at[:, 0:128], gate_out, sem.at[0]),
        pltpu.make_async_copy(wgu.at[:, 128:256], up_out, sem.at[1]),
        pltpu.make_async_copy(wd, down_out, sem.at[2]),
        pltpu.make_async_copy(mixed_ref, mixed_out, sem.at[3]),
    ]
    for cp in copies[:3]:
        cp.start()

    def returned(k, e):
        n = slots_of(k)
        both = rr[k, 2 * e, 0:n].astype(F32) + rr[k, 2 * e + 1, 0:n].astype(F32)
        if n == SLOT:
            return both
        return jnp.concatenate([both[:, : CW // 2], both[:, CW // 2 :]], axis=0)

    per_expert = jnp.concatenate(
        [
            jnp.concatenate([returned(k, e) for e in range(EXPERTS)], axis=0)
            for k in range(NC)
        ],
        axis=1,
    )
    mixed = lax.dot_general(
        wmix[...], per_expert, (((0,), (0,)), ((), ())),
        precision=lax.Precision.HIGHEST, preferred_element_type=F32,
    )
    mixed_ref[...] = jnp.concatenate(
        [
            mixed[:, NX * start + i * size : NX * start + (i + 1) * size]
            for i in range(NX)
            for start, size in CHUNKS
        ],
        axis=1,
    ).astype(BF16)
    copies[3].start()
    for cp in copies:
        cp.wait()


def per_device(tokens, routes, route_logits, norm_gain, gate_weight, up_weight, down_weight):
    dma = pltpu.SemaphoreType.DMA
    hbm = pl.BlockSpec(memory_space=pltpu.HBM)
    vmem = pl.BlockSpec(memory_space=pltpu.VMEM)
    held = pl.pallas_call(
        kernel,
        out_shape=(
            pltpu.VMEM((EXPERTS * SLOT, TOK), F32),
            pltpu.VMEM((NC, NZ, SLOT, CW), BF16),
            pltpu.VMEM((D, 256), BF16),
            pltpu.VMEM((NZ, NX, 128, 128), BF16),
        ),
        in_specs=[hbm] * 7,
        out_specs=(vmem,) * 4,
        scratch_shapes=[
            pltpu.VMEM((TOK, D), BF16),
            pltpu.VMEM((2, TOK), jnp.int32),
            pltpu.VMEM((2, TOK), F32),
            pltpu.VMEM((1, 128), F32),
            pltpu.VMEM((3, EXPERTS, 128, 1024), F32),
            pltpu.VMEM((EXPERTS, SLOT, KB), BF16),
            pltpu.VMEM((NFS, 128, 256), BF16),
            pltpu.VMEM((NFS, 128, 128), BF16),
            pltpu.VMEM((NTP, ROWS, KB), BF16),
            pltpu.VMEM((NTP, ROWS, 128), BF16),
            pltpu.VMEM((NC, NTP, NX, DR, 128), BF16),
            pltpu.VMEM((NC, NX, XROWS, CW), BF16),
            pltpu.VMEM((NC, NX - 1, XROWS, CW), BF16),
            pltpu.VMEM((NC, NZ, SLOT, CW), BF16),
            dma((4,)), dma((3,)),
            dma, dma((NZ,)), dma, dma((NX - 1,)), dma, dma((3, NX)), dma, dma, dma,
            pltpu.SemaphoreType.REGULAR,
            dma, dma, dma((NC,)), dma((NC,)), dma, dma((3, 2)), dma, dma,
            dma((NC,)), dma((NC,)), dma((NC,)), dma((NC,)), dma((NC,)), dma((NC,)),
        ],
        compiler_params=pltpu.CompilerParams(
            collective_id=0, has_side_effects=True, vmem_limit_bytes=48 * 2**20
        ),
        name="expert_handover",
    )(
        *(
            pltpu.with_memory_space_constraint(a, pltpu.HBM)
            for a in (
                tokens, routes.T, route_logits.T, norm_gain[None, :],
                gate_weight, up_weight, down_weight,
            )
        )
    )
    gate, up, down, mixed = pl.pallas_call(
        write_out,
        out_shape=(
            jax.ShapeDtypeStruct((D, 128), BF16),
            jax.ShapeDtypeStruct((D, 128), BF16),
            jax.ShapeDtypeStruct((NZ, NX, 128, 128), BF16),
            jax.ShapeDtypeStruct((TOK, KB), BF16),
        ),
        in_specs=[vmem] * 4,
        out_specs=(hbm, hbm, hbm, hbm),
        scratch_shapes=[pltpu.VMEM((TOK, KB), BF16), dma((4,))],
        compiler_params=pltpu.CompilerParams(vmem_limit_bytes=6 * 2**20),
        name="write_out",
    )(*(pltpu.with_memory_space_constraint(a, pltpu.VMEM) for a in held))
    return (mixed, gate[None], up[None], down.reshape(1, D, 128))


def solution(mesh):
    in_specs = (
        P("fs", None),
        P("fs", None),
        P("fs", None),
        P("fs"),
        P(None, "fs", "tp"),
        P(None, "fs", "tp"),
        P(None, "fs", "tp"),
    )
    out_specs = (P("fs", "tp"), P("tp", None, "fs"), P("tp", None, "fs"), P("tp", None, "fs"))
    return jax.shard_map(
        per_device, mesh=mesh, in_specs=in_specs, out_specs=out_specs, check_vma=False
    )
```

```python
import functools

import jax
import jax.numpy as jnp
from jax import lax
from jax.experimental import pallas as pl
from jax.experimental.pallas import tpu as pltpu
from jax.sharding import PartitionSpec as P

MESH = pl.DeviceIdType.MESH
NZ, NX, NY = 8, 4, 4
NFS, NTP = 32, 8
EXPERTS = 4
D = 4096
KB = D // NTP
TOK = 40
SLOT = 32
ROWS = NFS * SLOT
XROWS = NZ * SLOT
CHUNKS = ((0, 32), (32, 32), (64, 16), (80, 16), (96, 16), (112, 16))
NC = len(CHUNKS)
DR = 32
CW = NX * DR
F32, BF16 = jnp.float32, jnp.bfloat16


def rem(a, n):
    return lax.rem(a, jnp.int32(n))


def div(a, n):
    return lax.div(a, jnp.int32(n))


def slots_of(k):
    return SLOT * CHUNKS[k][1] // DR


def kernel(
    tok_hbm, routes_hbm, logits_hbm, gain_hbm, gate_hbm, up_hbm, down_hbm,
    wmix, rr, wgu, wd,
    tok, routes_ref, logits_ref, gain_ref, stage, p_send, sg, sd, xg, hid, dn, ro, r1, r2,
    tok_sem, load_sem,
    t1_s, t1_r, t2_s, t2_r, t3_s, t3_r, t3f_s, cc_s, cc_r,
    go, gu_s, gu_r, wd_s, wd_r, h_s, h_r, hc_s, hc_r, dn_s, dn_r, r1_s, r1_r, r2_s, r2_r,
):
    fs, tp = lax.axis_index("fs"), lax.axis_index("tp")
    z, x = div(fs, NX), rem(fs, NX)
    y, core = div(tp, 2), rem(tp, 2)

    def rcopy(src, dst, ssem, rsem, fs2, tp2):
        return pltpu.make_async_remote_copy(
            src_ref=src, dst_ref=dst, send_sem=ssem, recv_sem=rsem,
            device_id=(fs2, tp2), device_id_type=MESH,
        )

    def wait_for(sem, ref):
        pltpu.make_async_copy(ref, ref, sem).wait()

    def tp_of(dy):
        return rem(y + dy, NY) * 2 + core

    other = y * 2 + (1 - core)

    small = [
        pltpu.make_async_copy(src, dst, tok_sem.at[i])
        for i, (src, dst) in enumerate(
            ((routes_hbm, routes_ref), (logits_hbm, logits_ref), (tok_hbm, tok), (gain_hbm, gain_ref))
        )
    ]
    for cp in small:
        cp.start()
    loads = []
    for m, hbm in enumerate((gate_hbm, up_hbm, down_hbm)):
        cp = pltpu.make_async_copy(hbm, stage.at[m], load_sem.at[m])
        cp.start()
        loads.append(cp)

    bar = pltpu.get_barrier_semaphore()

    @pl.loop(1, NFS)
    def _(i):
        pl.semaphore_signal(bar, inc=1, device_id=(rem(fs + i, NFS), tp), device_id_type=MESH)

    @pl.loop(1, NTP)
    def _(i):
        pl.semaphore_signal(bar, inc=1, device_id=(fs, rem(tp + i, NTP)), device_id_type=MESH)

    small[0].wait()
    small[1].wait()
    row = lax.broadcasted_iota(jnp.int32, (EXPERTS * SLOT, TOK), 0)
    row_e = div(row, SLOT)
    row_s = rem(row, SLOT).astype(F32)
    pick0 = jnp.where(routes_ref[0:1, :] == row_e, 1.0, 0.0).astype(F32)
    pick1 = jnp.where(routes_ref[1:2, :] == row_e, 1.0, 0.0).astype(F32)
    member = pick0 + pick1
    row_i = lax.broadcasted_iota(jnp.int32, (TOK, TOK), 0)
    col_i = lax.broadcasted_iota(jnp.int32, (TOK, TOK), 1)
    before = jnp.where(row_i < col_i, 1.0, 0.0).astype(BF16)
    position = jnp.dot(member.astype(BF16), before, preferred_element_type=F32)
    placing = jnp.where((position == row_s) & (member > 0.0), 1.0, 0.0).astype(F32)
    diff = logits_ref[0:1, :] - logits_ref[1:2, :]
    share0 = 1.0 / (1.0 + jnp.exp(-diff))
    share1 = 1.0 / (1.0 + jnp.exp(diff))
    wmix[...] = placing * (pick0 * share0 + pick1 * share1)

    small[2].wait()
    tf = tok[...].astype(F32)
    inv = lax.rsqrt(jnp.mean(tf * tf, axis=1, keepdims=True) + 1e-05)
    block = tok[:, pl.ds(pl.multiple_of(tp * KB, KB), KB)].astype(F32)
    normed = (block * inv).astype(BF16)
    packed = jnp.dot(placing.astype(BF16), normed, preferred_element_type=F32)
    p_send[...] = packed.astype(BF16).reshape(EXPERTS, SLOT, KB)
    own_x = pl.multiple_of(x * XROWS, XROWS)
    own_row = pl.multiple_of(x * XROWS + z * SLOT, SLOT)
    xg[tp, pl.ds(own_row, SLOT), :] = p_send[div(z, 2)]

    pl.semaphore_wait(bar, NFS - 1 + NTP - 1)

    for dz in (4, 3, 5, 2, 6, 1, 7):
        z2 = rem(z + dz, NZ)
        rcopy(
            p_send.at[div(z2, 2)], xg.at[tp, pl.ds(own_row, SLOT), :], t1_s, t1_r.at[dz],
            z2 * NX + x, tp,
        ).start()

    my_rows = pl.ds(pl.multiple_of(fs * 128, 128), 128)

    def send_gu(dz, dx):
        f2 = rem(z + dz, NZ) * NX + rem(x + dx, NX)
        rcopy(sg.at[f2], wgu.at[my_rows, :], gu_s, gu_r, f2, tp).start()

    def send_down(k, i):
        dx, dz = div(i, NZ), rem(i, NZ)
        f2 = rem(z + dz, NZ) * NX + rem(x + dx, NX)
        part = pl.ds(*CHUNKS[k])
        rcopy(
            sd.at[f2, part, :], wd.at[z, x, part, :], wd_s.at[k], wd_r.at[k], f2, tp
        ).start()

    small[3].wait()
    gain = jnp.transpose(jnp.broadcast_to(gain_ref[...], (128, 128)))
    for m in range(2):
        loads[m].wait()

        @pl.loop(0, EXPERTS)
        def _(e):
            for s in range(8):
                sg[e * 8 + s, :, m * 128 : (m + 1) * 128] = (
                    stage[m, e, :, s * 128 : (s + 1) * 128] * gain
                ).astype(BF16)

    wgu[pl.ds(pl.multiple_of(fs * 128, 128), 128), :] = sg[fs]

    @pl.loop(1, NZ)
    def _(dz):
        send_gu(dz, 0)

    loads[2].wait()

    @pl.loop(0, EXPERTS)
    def _(e):
        for s in range(8):
            sd[e * 8 + s] = stage[2, e, :, s * 128 : (s + 1) * 128].astype(BF16)

    wd[z, x] = sd[fs]

    def along_x(dz):
        piece = xg.at[tp, pl.ds(own_x + rem(z + NZ - dz, NZ) * SLOT, SLOT), :]
        if dz:
            wait_for(t1_r.at[dz], piece)
        for dx in (1, 3, 2):
            rcopy(
                piece, piece, t2_s, t2_r.at[dx - 1], z * NX + rem(x + dx, NX), tp
            ).start()

    for dz in (0, 1, 7, 2, 6, 3, 5, 4):
        along_x(dz)

    def part_of(t, p, half=None):
        base = rem(x + NX - p, NX) * XROWS
        if half is None:
            return xg.at[t, pl.ds(pl.multiple_of(base, XROWS), XROWS), :]
        h = XROWS // 2
        return xg.at[t, pl.ds(pl.multiple_of(base + half * h, h), h), :]

    def to_core(t, p):
        ref = part_of(t, p)
        rcopy(ref, ref, cc_s, cc_r, fs, other).start()

    def own_part(p):
        ref = part_of(tp, p)
        rcopy(ref, ref, t3_s, t3_r.at[0, p], fs, tp_of(1)).start()
        rcopy(ref, ref, t3_s, t3_r.at[1, p], fs, tp_of(3)).start()
        to_core(tp, p)

    own_part(0)

    def send_gu_from(dx):
        @pl.loop(0, NZ)
        def _(dz):
            send_gu(dz, dx)

    for p in range(1, NX):
        wait_for(t2_r.at[p - 1], part_of(tp, p))
        own_part(p)
        send_gu_from(p)
    def send_chunks(first, end):
        for k in range(first, end):

            @pl.loop(1, NFS)
            def _(i):
                send_down(k, i)

    @pl.when(core == 0)
    def _():
        send_chunks(0, NC)

    for p in range(NX):
        below, above = tp_of(3), tp_of(1)
        ref = part_of(below, p)
        wait_for(t3_r.at[0, p], ref)
        half = part_of(below, p, 0)
        rcopy(half, half, t3f_s, t3_r.at[2, p], fs, above).start()
        to_core(below, p)
        ref = part_of(above, p)
        wait_for(t3_r.at[1, p], ref)
        half = part_of(above, p, 1)
        rcopy(half, half, t3f_s, t3_r.at[2, p], fs, below).start()
        to_core(above, p)
    for p in range(NX):
        wait_for(t3_r.at[2, p], part_of(tp_of(2), p))
        to_core(tp_of(2), p)
    wait_for(cc_r, xg.at[0:NY])

    @pl.when(core == 0)
    def _():
        wait_for(gu_s, wgu.at[0 : (NFS - 1) * 128, :])
        pl.semaphore_signal(go, inc=1, device_id=(fs, other), device_id_type=MESH)

    wait_for(gu_r, wgu.at[0 : (NFS - 1) * 128, :])

    @pl.when(core == 1)
    def _():
        send_chunks(0, 1)


    @pl.loop(0, NX)
    def _(r):
        rows = pl.ds(pl.multiple_of(r * XROWS, XROWS), XROWS)
        acc = jnp.zeros((XROWS, 256), F32)
        for t in range(NTP):
            acc += jnp.dot(
                xg[t, rows, :], wgu[t * KB : (t + 1) * KB, :], preferred_element_type=F32
            )
        g, u = acc[:, 0:128], acc[:, 128:256]
        hid[tp, rows, :] = (g / (1.0 + jnp.exp(-g)) * u).astype(BF16)

    def lanes_of(t):
        return hid.at[t]

    half = ROWS // 2

    def piece_of(t, h):
        return hid.at[t, h * half : (h + 1) * half, :]

    below, above = tp_of(3), tp_of(1)
    for h in (0, 1):
        up_piece, down_piece = piece_of(tp, h), piece_of(tp, 1 - h)
        rcopy(up_piece, up_piece, h_s, h_r.at[0, h], fs, above).start()
        rcopy(down_piece, down_piece, h_s, h_r.at[1, 1 - h], fs, below).start()
    own_h = lanes_of(tp)
    rcopy(own_h, own_h, hc_s, hc_r, fs, other).start()

    def h_core(t):
        rcopy(lanes_of(t), lanes_of(t), hc_s, hc_r, fs, other).start()

    def summed(k):
        n = slots_of(k)
        wait_for(r1_r.at[k], r1.at[k, :, 0 : NZ * n])
        total = ro[k, x, 0 : NZ * n].astype(F32)
        for i in range(NX - 1):
            total += r1[k, i, 0 : NZ * n].astype(F32)
        r2[k, :, 0:n] = total.astype(BF16).reshape(NZ, n, CW)
        rr[k, z, 0:n] = r2[k, z, 0:n]

        @pl.loop(1, NZ)
        def _(dz):
            z2 = rem(z + dz, NZ)
            rcopy(
                r2.at[k, z2, 0:n], rr.at[k, z, 0:n], r2_s.at[k], r2_r.at[k], z2 * NX + x, tp
            ).start()

    def forward(k):
        start, size = CHUNKS[k]
        part = slice(start, start + size)
        wait_for(wd_r.at[k], sd.at[0 : NFS - 1, 0:size, :])

        @pl.loop(1, NTP)
        def _(i):
            to = rem(tp + i, NTP)
            rcopy(
                wd.at[to, :, part, :], dn.at[k, tp, :, 0:size, :], dn_s.at[k], dn_r.at[k], fs, to
            ).start()

        dn[k, tp, :, 0:size, :] = wd[tp, :, part, :]

    def project(k):
        size, n = CHUNKS[k][1], slots_of(k)
        wait_for(dn_r.at[k], sd.at[0 : 4 * (NTP - 1), 0:size, :])
        dnk = jnp.concatenate(
            [dn[k, t, :, 0:size, :].reshape(NX * size, 128) for t in range(NTP)], axis=1
        )
        for j in (1, 2, 3, 0):
            x2 = rem(x + j, NX)
            rows = pl.ds(pl.multiple_of(x2 * XROWS, XROWS), XROWS)
            out = lax.dot_general(
                jnp.concatenate([hid[t, rows, :] for t in range(NTP)], axis=1),
                dnk, (((1,), (1,)), ((), ())), preferred_element_type=F32,
            )
            if n < SLOT:
                out = out.reshape(NZ, 2, n, NX * size)
                out = jnp.concatenate([out[:, 0], out[:, 1]], axis=-1).reshape(NZ * n, CW)
            ro[k, x2, 0 : NZ * n] = out.astype(BF16)
        for j in (1, 2, 3):
            x2 = rem(x + j, NX)
            rcopy(
                ro.at[k, x2, 0 : NZ * n], r1.at[k, j - 1, 0 : NZ * n], r1_s.at[k], r1_r.at[k],
                z * NX + x2, tp,
            ).start()

    @pl.when(core == 1)
    def _():
        pl.semaphore_wait(go, 1)
        send_chunks(1, NC)
        wait_for(gu_s, wgu.at[0 : (NFS - 1) * 128, :])

    def relay_near():
        wait_for(h_r.at[0, 0], piece_of(below, 0))
        rcopy(piece_of(below, 0), piece_of(below, 0), h_s, h_r.at[2, 0], fs, above).start()
        wait_for(h_r.at[1, 1], piece_of(above, 1))
        rcopy(piece_of(above, 1), piece_of(above, 1), h_s, h_r.at[2, 0], fs, below).start()
        wait_for(h_r.at[0, 1], piece_of(below, 1))
        h_core(below)
        wait_for(h_r.at[1, 0], piece_of(above, 0))
        h_core(above)

    def relay_far():
        wait_for(h_r.at[2, 0], lanes_of(tp_of(2)))
        h_core(tp_of(2))

    @pl.when(core == 0)
    def _():
        forward(0)
        relay_near()
        forward(1)
        relay_far()
        forward(2)

    @pl.when(core == 1)
    def _():
        relay_near()
        relay_far()
        forward(0)
        forward(1)

    wait_for(hc_r, hid.at[0:NY])
    project(0)

    @pl.when(core == 1)
    def _():
        forward(2)

    forward(3)
    project(1)
    forward(4)
    project(2)
    summed(0)
    forward(5)
    project(3)
    summed(1)
    project(4)
    summed(2)
    project(5)
    summed(3)
    summed(4)
    summed(5)

    for k in range(NC):
        wait_for(r2_r.at[k], r2.at[k, 0 : NZ - 1, 0 : slots_of(k)])

    wait_for(t1_s, xg.at[0, 0 : (NZ - 1) * SLOT, :])
    wait_for(t2_s, xg.at[0, 0 : (NX - 1) * XROWS, :])
    wait_for(t3_s, xg.at[0:2])
    wait_for(t3f_s, xg.at[0])
    wait_for(cc_s, xg.at[0:NY])
    wait_for(h_s, hid.at[0 : NY - 1])
    wait_for(hc_s, hid.at[0:NY])
    for k in range(NC):
        size, n = CHUNKS[k][1], slots_of(k)
        wait_for(wd_s.at[k], sd.at[0 : NFS - 1, 0:size, :])
        wait_for(dn_s.at[k], sd.at[0 : 4 * (NTP - 1), 0:size, :])
        wait_for(r1_s.at[k], r1.at[k, :, 0 : NZ * n])
        wait_for(r2_s.at[k], r2.at[k, 0 : NZ - 1, 0:n])


def write_out(wmix, rr, wgu, wd, gate_out, up_out, down_out, mixed_out, mixed_ref, sem):
    copies = [
        pltpu.make_async_copy(wgu.at[:, 0:128], gate_out, sem.at[0]),
        pltpu.make_async_copy(wgu.at[:, 128:256], up_out, sem.at[1]),
        pltpu.make_async_copy(wd, down_out, sem.at[2]),
        pltpu.make_async_copy(mixed_ref, mixed_out, sem.at[3]),
    ]
    for cp in copies[:3]:
        cp.start()

    def returned(k, e):
        n = slots_of(k)
        both = rr[k, 2 * e, 0:n].astype(F32) + rr[k, 2 * e + 1, 0:n].astype(F32)
        if n == SLOT:
            return both
        return jnp.concatenate([both[:, : CW // 2], both[:, CW // 2 :]], axis=0)

    per_expert = jnp.concatenate(
        [
            jnp.concatenate([returned(k, e) for e in range(EXPERTS)], axis=0)
            for k in range(NC)
        ],
        axis=1,
    )
    mixed = lax.dot_general(
        wmix[...], per_expert, (((0,), (0,)), ((), ())),
        precision=lax.Precision.HIGHEST, preferred_element_type=F32,
    )
    mixed_ref[...] = jnp.concatenate(
        [
            mixed[:, NX * start + i * size : NX * start + (i + 1) * size]
            for i in range(NX)
            for start, size in CHUNKS
        ],
        axis=1,
    ).astype(BF16)
    copies[3].start()
    for cp in copies:
        cp.wait()


def per_device(tokens, routes, route_logits, norm_gain, gate_weight, up_weight, down_weight):
    dma = pltpu.SemaphoreType.DMA
    hbm = pl.BlockSpec(memory_space=pltpu.HBM)
    vmem = pl.BlockSpec(memory_space=pltpu.VMEM)
    held = pl.pallas_call(
        kernel,
        out_shape=(
            pltpu.VMEM((EXPERTS * SLOT, TOK), F32),
            pltpu.VMEM((NC, NZ, SLOT, CW), BF16),
            pltpu.VMEM((D, 256), BF16),
            pltpu.VMEM((NZ, NX, 128, 128), BF16),
        ),
        in_specs=[hbm] * 7,
        out_specs=(vmem,) * 4,
        scratch_shapes=[
            pltpu.VMEM((TOK, D), BF16),
            pltpu.VMEM((2, TOK), jnp.int32),
            pltpu.VMEM((2, TOK), F32),
            pltpu.VMEM((1, 128), F32),
            pltpu.VMEM((3, EXPERTS, 128, 1024), F32),
            pltpu.VMEM((EXPERTS, SLOT, KB), BF16),
            pltpu.VMEM((NFS, 128, 256), BF16),
            pltpu.VMEM((NFS, 128, 128), BF16),
            pltpu.VMEM((NTP, ROWS, KB), BF16),
            pltpu.VMEM((NTP, ROWS, 128), BF16),
            pltpu.VMEM((NC, NTP, NX, DR, 128), BF16),
            pltpu.VMEM((NC, NX, XROWS, CW), BF16),
            pltpu.VMEM((NC, NX - 1, XROWS, CW), BF16),
            pltpu.VMEM((NC, NZ, SLOT, CW), BF16),
            dma((4,)), dma((3,)),
            dma, dma((NZ,)), dma, dma((NX - 1,)), dma, dma((3, NX)), dma, dma, dma,
            pltpu.SemaphoreType.REGULAR,
            dma, dma, dma((NC,)), dma((NC,)), dma, dma((3, 2)), dma, dma,
            dma((NC,)), dma((NC,)), dma((NC,)), dma((NC,)), dma((NC,)), dma((NC,)),
        ],
        compiler_params=pltpu.CompilerParams(
            collective_id=0, has_side_effects=True, vmem_limit_bytes=48 * 2**20
        ),
        name="expert_handover",
    )(
        *(
            pltpu.with_memory_space_constraint(a, pltpu.HBM)
            for a in (
                tokens, routes.T, route_logits.T, norm_gain[None, :],
                gate_weight, up_weight, down_weight,
            )
        )
    )
    gate, up, down, mixed = pl.pallas_call(
        write_out,
        out_shape=(
            jax.ShapeDtypeStruct((D, 128), BF16),
            jax.ShapeDtypeStruct((D, 128), BF16),
            jax.ShapeDtypeStruct((NZ, NX, 128, 128), BF16),
            jax.ShapeDtypeStruct((TOK, KB), BF16),
        ),
        in_specs=[vmem] * 4,
        out_specs=(hbm, hbm, hbm, hbm),
        scratch_shapes=[pltpu.VMEM((TOK, KB), BF16), dma((4,))],
        compiler_params=pltpu.CompilerParams(vmem_limit_bytes=6 * 2**20),
        name="write_out",
    )(*(pltpu.with_memory_space_constraint(a, pltpu.VMEM) for a in held))
    return (mixed, gate[None], up[None], down.reshape(1, D, 128))


def solution(mesh):
    in_specs = (
        P("fs", None),
        P("fs", None),
        P("fs", None),
        P("fs"),
        P(None, "fs", "tp"),
        P(None, "fs", "tp"),
        P(None, "fs", "tp"),
    )
    out_specs = (P("fs", "tp"), P("tp", None, "fs"), P("tp", None, "fs"), P("tp", None, "fs"))
    return jax.shard_map(
        per_device, mesh=mesh, in_specs=in_specs, out_specs=out_specs, check_vma=False
    )
```

```python
import functools

import jax
import jax.numpy as jnp
from jax import lax
from jax.experimental import pallas as pl
from jax.experimental.pallas import tpu as pltpu
from jax.sharding import PartitionSpec as P

MESH = pl.DeviceIdType.MESH
NZ, NX, NY = 8, 4, 4
NFS, NTP = 32, 8
EXPERTS = 4
D = 4096
KB = D // NTP
TOK = 40
SLOT = 32
ROWS = NFS * SLOT
XROWS = NZ * SLOT
CHUNKS = ((0, 32), (32, 32), (64, 16), (80, 16), (96, 16), (112, 16))
NC = len(CHUNKS)
DR = 32
CW = NX * DR
F32, BF16 = jnp.float32, jnp.bfloat16


def rem(a, n):
    return lax.rem(a, jnp.int32(n))


def div(a, n):
    return lax.div(a, jnp.int32(n))


def slots_of(k):
    return SLOT * CHUNKS[k][1] // DR


def kernel(
    tok_hbm, routes_hbm, logits_hbm, gain_hbm, gate_hbm, up_hbm, down_hbm,
    wmix, rr, wgu, wd,
    tok, routes_ref, logits_ref, gain_ref, stage, p_send, sg, sd, xg, hid, dn, ro, r1, r2,
    tok_sem, load_sem,
    t1_s, t1_r, t2_s, t2_r, t3_s, t3_r, t3f_s, cc_s, cc_r,
    go, gu_s, gu_r, wd_s, wd_r, h_s, h_r, hc_s, hc_r, dn_s, dn_r, r1_s, r1_r, r2_s, r2_r,
):
    fs, tp = lax.axis_index("fs"), lax.axis_index("tp")
    z, x = div(fs, NX), rem(fs, NX)
    y, core = div(tp, 2), rem(tp, 2)

    def rcopy(src, dst, ssem, rsem, fs2, tp2):
        return pltpu.make_async_remote_copy(
            src_ref=src, dst_ref=dst, send_sem=ssem, recv_sem=rsem,
            device_id=(fs2, tp2), device_id_type=MESH,
        )

    def wait_for(sem, ref):
        pltpu.make_async_copy(ref, ref, sem).wait()

    def tp_of(dy):
        return rem(y + dy, NY) * 2 + core

    other = y * 2 + (1 - core)

    small = [
        pltpu.make_async_copy(src, dst, tok_sem.at[i])
        for i, (src, dst) in enumerate(
            ((routes_hbm, routes_ref), (logits_hbm, logits_ref), (tok_hbm, tok), (gain_hbm, gain_ref))
        )
    ]
    for cp in small:
        cp.start()
    loads = []
    for m, hbm in enumerate((gate_hbm, up_hbm, down_hbm)):
        cp = pltpu.make_async_copy(hbm, stage.at[m], load_sem.at[m])
        cp.start()
        loads.append(cp)

    bar = pltpu.get_barrier_semaphore()

    @pl.loop(1, NFS)
    def _(i):
        pl.semaphore_signal(bar, inc=1, device_id=(rem(fs + i, NFS), tp), device_id_type=MESH)

    @pl.loop(1, NTP)
    def _(i):
        pl.semaphore_signal(bar, inc=1, device_id=(fs, rem(tp + i, NTP)), device_id_type=MESH)

    small[0].wait()
    small[1].wait()
    row = lax.broadcasted_iota(jnp.int32, (EXPERTS * SLOT, TOK), 0)
    row_e = div(row, SLOT)
    row_s = rem(row, SLOT).astype(F32)
    pick0 = jnp.where(routes_ref[0:1, :] == row_e, 1.0, 0.0).astype(F32)
    pick1 = jnp.where(routes_ref[1:2, :] == row_e, 1.0, 0.0).astype(F32)
    member = pick0 + pick1
    row_i = lax.broadcasted_iota(jnp.int32, (TOK, TOK), 0)
    col_i = lax.broadcasted_iota(jnp.int32, (TOK, TOK), 1)
    before = jnp.where(row_i < col_i, 1.0, 0.0).astype(BF16)
    position = jnp.dot(member.astype(BF16), before, preferred_element_type=F32)
    placing = jnp.where((position == row_s) & (member > 0.0), 1.0, 0.0).astype(F32)
    diff = logits_ref[0:1, :] - logits_ref[1:2, :]
    share0 = 1.0 / (1.0 + jnp.exp(-diff))
    share1 = 1.0 / (1.0 + jnp.exp(diff))
    wmix[...] = placing * (pick0 * share0 + pick1 * share1)

    small[2].wait()
    tf = tok[...].astype(F32)
    inv = lax.rsqrt(jnp.mean(tf * tf, axis=1, keepdims=True) + 1e-05)
    block = tok[:, pl.ds(pl.multiple_of(tp * KB, KB), KB)].astype(F32)
    normed = (block * inv).astype(BF16)
    packed = jnp.dot(placing.astype(BF16), normed, preferred_element_type=F32)
    p_send[...] = packed.astype(BF16).reshape(EXPERTS, SLOT, KB)
    own_x = pl.multiple_of(x * XROWS, XROWS)
    own_row = pl.multiple_of(x * XROWS + z * SLOT, SLOT)
    xg[tp, pl.ds(own_row, SLOT), :] = p_send[div(z, 2)]

    pl.semaphore_wait(bar, NFS - 1 + NTP - 1)

    for dz in (4, 3, 5, 2, 6, 1, 7):
        z2 = rem(z + dz, NZ)
        rcopy(
            p_send.at[div(z2, 2)], xg.at[tp, pl.ds(own_row, SLOT), :], t1_s, t1_r.at[dz],
            z2 * NX + x, tp,
        ).start()

    my_rows = pl.ds(pl.multiple_of(fs * 128, 128), 128)

    def send_gu(dz, dx):
        f2 = rem(z + dz, NZ) * NX + rem(x + dx, NX)
        rcopy(sg.at[f2], wgu.at[my_rows, :], gu_s, gu_r, f2, tp).start()

    def send_down(k, i):
        dx, dz = div(i, NZ), rem(i, NZ)
        f2 = rem(z + dz, NZ) * NX + rem(x + dx, NX)
        part = pl.ds(*CHUNKS[k])
        rcopy(
            sd.at[f2, part, :], wd.at[z, x, part, :], wd_s.at[k], wd_r.at[k], f2, tp
        ).start()

    small[3].wait()
    gain = jnp.transpose(jnp.broadcast_to(gain_ref[...], (128, 128)))
    for m in range(2):
        loads[m].wait()

        @pl.loop(0, EXPERTS)
        def _(e):
            for s in range(8):
                sg[e * 8 + s, :, m * 128 : (m + 1) * 128] = (
                    stage[m, e, :, s * 128 : (s + 1) * 128] * gain
                ).astype(BF16)

    wgu[pl.ds(pl.multiple_of(fs * 128, 128), 128), :] = sg[fs]

    @pl.loop(1, NZ)
    def _(dz):
        send_gu(dz, 0)

    loads[2].wait()

    @pl.loop(0, EXPERTS)
    def _(e):
        for s in range(8):
            sd[e * 8 + s] = stage[2, e, :, s * 128 : (s + 1) * 128].astype(BF16)

    wd[z, x] = sd[fs]

    def along_x(dz):
        piece = xg.at[tp, pl.ds(own_x + rem(z + NZ - dz, NZ) * SLOT, SLOT), :]
        if dz:
            wait_for(t1_r.at[dz], piece)
        for dx in (1, 3, 2):
            rcopy(
                piece, piece, t2_s, t2_r.at[dx - 1], z * NX + rem(x + dx, NX), tp
            ).start()

    for dz in (0, 1, 7, 2, 6, 3, 5, 4):
        along_x(dz)

    def part_of(t, p, half=None):
        base = rem(x + NX - p, NX) * XROWS
        if half is None:
            return xg.at[t, pl.ds(pl.multiple_of(base, XROWS), XROWS), :]
        h = XROWS // 2
        return xg.at[t, pl.ds(pl.multiple_of(base + half * h, h), h), :]

    def to_core(t, p):
        ref = part_of(t, p)
        rcopy(ref, ref, cc_s, cc_r, fs, other).start()

    def own_part(p):
        ref = part_of(tp, p)
        rcopy(ref, ref, t3_s, t3_r.at[0, p], fs, tp_of(1)).start()
        rcopy(ref, ref, t3_s, t3_r.at[1, p], fs, tp_of(3)).start()
        to_core(tp, p)

    own_part(0)

    def send_gu_from(dx):
        @pl.loop(0, NZ)
        def _(dz):
            send_gu(dz, dx)

    for p in range(1, NX):
        wait_for(t2_r.at[p - 1], part_of(tp, p))
        own_part(p)
        send_gu_from(p)
    def send_chunks(first, end):
        for k in range(first, end):

            @pl.loop(1, NFS)
            def _(i):
                send_down(k, i)

    @pl.when(core == 0)
    def _():
        send_chunks(0, NC)

    for p in range(NX):
        below, above = tp_of(3), tp_of(1)
        ref = part_of(below, p)
        wait_for(t3_r.at[0, p], ref)
        half = part_of(below, p, 0)
        rcopy(half, half, t3f_s, t3_r.at[2, p], fs, above).start()
        to_core(below, p)
        ref = part_of(above, p)
        wait_for(t3_r.at[1, p], ref)
        half = part_of(above, p, 1)
        rcopy(half, half, t3f_s, t3_r.at[2, p], fs, below).start()
        to_core(above, p)
    for p in range(NX):
        wait_for(t3_r.at[2, p], part_of(tp_of(2), p))
        to_core(tp_of(2), p)
    wait_for(cc_r, xg.at[0:NY])

    @pl.when(core == 0)
    def _():
        wait_for(gu_s, wgu.at[0 : (NFS - 1) * 128, :])
        pl.semaphore_signal(go, inc=1, device_id=(fs, other), device_id_type=MESH)

    wait_for(gu_r, wgu.at[0 : (NFS - 1) * 128, :])

    @pl.when(core == 1)
    def _():
        send_chunks(0, 1)


    @pl.loop(0, NX)
    def _(r):
        rows = pl.ds(pl.multiple_of(r * XROWS, XROWS), XROWS)
        acc = jnp.zeros((XROWS, 256), F32)
        for t in range(NTP):
            acc += jnp.dot(
                xg[t, rows, :], wgu[t * KB : (t + 1) * KB, :], preferred_element_type=F32
            )
        g, u = acc[:, 0:128], acc[:, 128:256]
        hid[tp, rows, :] = (g / (1.0 + jnp.exp(-g)) * u).astype(BF16)

    def lanes_of(t):
        return hid.at[t]

    half = ROWS // 2

    def piece_of(t, h):
        return hid.at[t, h * half : (h + 1) * half, :]

    below, above = tp_of(3), tp_of(1)
    for h in (0, 1):
        up_piece, down_piece = piece_of(tp, h), piece_of(tp, 1 - h)
        rcopy(up_piece, up_piece, h_s, h_r.at[0, h], fs, above).start()
        rcopy(down_piece, down_piece, h_s, h_r.at[1, 1 - h], fs, below).start()
    own_h = lanes_of(tp)
    rcopy(own_h, own_h, hc_s, hc_r, fs, other).start()

    def h_core(t):
        rcopy(lanes_of(t), lanes_of(t), hc_s, hc_r, fs, other).start()

    def summed(k):
        n = slots_of(k)
        wait_for(r1_r.at[k], r1.at[k, :, 0 : NZ * n])
        total = ro[k, x, 0 : NZ * n].astype(F32)
        for i in range(NX - 1):
            total += r1[k, i, 0 : NZ * n].astype(F32)
        r2[k, :, 0:n] = total.astype(BF16).reshape(NZ, n, CW)
        rr[k, z, 0:n] = r2[k, z, 0:n]

        @pl.loop(1, NZ)
        def _(dz):
            z2 = rem(z + dz, NZ)
            rcopy(
                r2.at[k, z2, 0:n], rr.at[k, z, 0:n], r2_s.at[k], r2_r.at[k], z2 * NX + x, tp
            ).start()

    def forward(k):
        start, size = CHUNKS[k]
        part = slice(start, start + size)
        wait_for(wd_r.at[k], sd.at[0 : NFS - 1, 0:size, :])

        @pl.loop(1, NTP)
        def _(i):
            to = rem(tp + i, NTP)
            rcopy(
                wd.at[to, :, part, :], dn.at[k, tp, :, 0:size, :], dn_s.at[k], dn_r.at[k], fs, to
            ).start()

        dn[k, tp, :, 0:size, :] = wd[tp, :, part, :]

    def project(k):
        size, n = CHUNKS[k][1], slots_of(k)
        wait_for(dn_r.at[k], sd.at[0 : 4 * (NTP - 1), 0:size, :])
        dnk = jnp.concatenate(
            [dn[k, t, :, 0:size, :].reshape(NX * size, 128) for t in range(NTP)], axis=1
        )
        for j in (1, 2, 3, 0):
            x2 = rem(x + j, NX)
            rows = pl.ds(pl.multiple_of(x2 * XROWS, XROWS), XROWS)
            out = lax.dot_general(
                jnp.concatenate([hid[t, rows, :] for t in range(NTP)], axis=1),
                dnk, (((1,), (1,)), ((), ())), preferred_element_type=F32,
            )
            if n < SLOT:
                out = out.reshape(NZ, 2, n, NX * size)
                out = jnp.concatenate([out[:, 0], out[:, 1]], axis=-1).reshape(NZ * n, CW)
            ro[k, x2, 0 : NZ * n] = out.astype(BF16)
        for j in (1, 2, 3):
            x2 = rem(x + j, NX)
            rcopy(
                ro.at[k, x2, 0 : NZ * n], r1.at[k, j - 1, 0 : NZ * n], r1_s.at[k], r1_r.at[k],
                z * NX + x2, tp,
            ).start()

    @pl.when(core == 1)
    def _():
        pl.semaphore_wait(go, 1)
        send_chunks(1, NC)
        wait_for(gu_s, wgu.at[0 : (NFS - 1) * 128, :])

    def relay_near():
        wait_for(h_r.at[0, 0], piece_of(below, 0))
        rcopy(piece_of(below, 0), piece_of(below, 0), h_s, h_r.at[2, 0], fs, above).start()
        wait_for(h_r.at[1, 1], piece_of(above, 1))
        rcopy(piece_of(above, 1), piece_of(above, 1), h_s, h_r.at[2, 0], fs, below).start()
        wait_for(h_r.at[0, 1], piece_of(below, 1))
        h_core(below)
        wait_for(h_r.at[1, 0], piece_of(above, 0))
        h_core(above)

    def relay_far():
        wait_for(h_r.at[2, 0], lanes_of(tp_of(2)))
        h_core(tp_of(2))

    @pl.when(core == 0)
    def _():
        forward(0)
        relay_near()
        forward(1)
        relay_far()
        forward(2)

    @pl.when(core == 1)
    def _():
        relay_near()
        relay_far()
        forward(0)
        forward(1)

    wait_for(hc_r, hid.at[0:NY])
    project(0)

    @pl.when(core == 1)
    def _():
        forward(2)

    forward(3)
    project(1)
    forward(4)
    project(2)
    summed(0)
    forward(5)
    project(3)
    project(4)
    summed(1)
    project(5)
    summed(2)
    summed(3)
    summed(4)
    summed(5)

    for k in range(NC):
        wait_for(r2_r.at[k], r2.at[k, 0 : NZ - 1, 0 : slots_of(k)])

    wait_for(t1_s, xg.at[0, 0 : (NZ - 1) * SLOT, :])
    wait_for(t2_s, xg.at[0, 0 : (NX - 1) * XROWS, :])
    wait_for(t3_s, xg.at[0:2])
    wait_for(t3f_s, xg.at[0])
    wait_for(cc_s, xg.at[0:NY])
    wait_for(h_s, hid.at[0 : NY - 1])
    wait_for(hc_s, hid.at[0:NY])
    for k in range(NC):
        size, n = CHUNKS[k][1], slots_of(k)
        wait_for(wd_s.at[k], sd.at[0 : NFS - 1, 0:size, :])
        wait_for(dn_s.at[k], sd.at[0 : 4 * (NTP - 1), 0:size, :])
        wait_for(r1_s.at[k], r1.at[k, :, 0 : NZ * n])
        wait_for(r2_s.at[k], r2.at[k, 0 : NZ - 1, 0:n])


def write_out(wmix, rr, wgu, wd, gate_out, up_out, down_out, mixed_out, mixed_ref, sem):
    copies = [
        pltpu.make_async_copy(wgu.at[:, 0:128], gate_out, sem.at[0]),
        pltpu.make_async_copy(wgu.at[:, 128:256], up_out, sem.at[1]),
        pltpu.make_async_copy(wd, down_out, sem.at[2]),
        pltpu.make_async_copy(mixed_ref, mixed_out, sem.at[3]),
    ]
    for cp in copies[:3]:
        cp.start()

    def returned(k, e):
        n = slots_of(k)
        both = rr[k, 2 * e, 0:n].astype(F32) + rr[k, 2 * e + 1, 0:n].astype(F32)
        if n == SLOT:
            return both
        return jnp.concatenate([both[:, : CW // 2], both[:, CW // 2 :]], axis=0)

    per_expert = jnp.concatenate(
        [
            jnp.concatenate([returned(k, e) for e in range(EXPERTS)], axis=0)
            for k in range(NC)
        ],
        axis=1,
    )
    mixed = lax.dot_general(
        wmix[...], per_expert, (((0,), (0,)), ((), ())),
        precision=lax.Precision.HIGHEST, preferred_element_type=F32,
    )
    mixed_ref[...] = jnp.concatenate(
        [
            mixed[:, NX * start + i * size : NX * start + (i + 1) * size]
            for i in range(NX)
            for start, size in CHUNKS
        ],
        axis=1,
    ).astype(BF16)
    copies[3].start()
    for cp in copies:
        cp.wait()


def per_device(tokens, routes, route_logits, norm_gain, gate_weight, up_weight, down_weight):
    dma = pltpu.SemaphoreType.DMA
    hbm = pl.BlockSpec(memory_space=pltpu.HBM)
    vmem = pl.BlockSpec(memory_space=pltpu.VMEM)
    held = pl.pallas_call(
        kernel,
        out_shape=(
            pltpu.VMEM((EXPERTS * SLOT, TOK), F32),
            pltpu.VMEM((NC, NZ, SLOT, CW), BF16),
            pltpu.VMEM((D, 256), BF16),
            pltpu.VMEM((NZ, NX, 128, 128), BF16),
        ),
        in_specs=[hbm] * 7,
        out_specs=(vmem,) * 4,
        scratch_shapes=[
            pltpu.VMEM((TOK, D), BF16),
            pltpu.VMEM((2, TOK), jnp.int32),
            pltpu.VMEM((2, TOK), F32),
            pltpu.VMEM((1, 128), F32),
            pltpu.VMEM((3, EXPERTS, 128, 1024), F32),
            pltpu.VMEM((EXPERTS, SLOT, KB), BF16),
            pltpu.VMEM((NFS, 128, 256), BF16),
            pltpu.VMEM((NFS, 128, 128), BF16),
            pltpu.VMEM((NTP, ROWS, KB), BF16),
            pltpu.VMEM((NTP, ROWS, 128), BF16),
            pltpu.VMEM((NC, NTP, NX, DR, 128), BF16),
            pltpu.VMEM((NC, NX, XROWS, CW), BF16),
            pltpu.VMEM((NC, NX - 1, XROWS, CW), BF16),
            pltpu.VMEM((NC, NZ, SLOT, CW), BF16),
            dma((4,)), dma((3,)),
            dma, dma((NZ,)), dma, dma((NX - 1,)), dma, dma((3, NX)), dma, dma, dma,
            pltpu.SemaphoreType.REGULAR,
            dma, dma, dma((NC,)), dma((NC,)), dma, dma((3, 2)), dma, dma,
            dma((NC,)), dma((NC,)), dma((NC,)), dma((NC,)), dma((NC,)), dma((NC,)),
        ],
        compiler_params=pltpu.CompilerParams(
            collective_id=0, has_side_effects=True, vmem_limit_bytes=48 * 2**20
        ),
        name="expert_handover",
    )(
        *(
            pltpu.with_memory_space_constraint(a, pltpu.HBM)
            for a in (
                tokens, routes.T, route_logits.T, norm_gain[None, :],
                gate_weight, up_weight, down_weight,
            )
        )
    )
    gate, up, down, mixed = pl.pallas_call(
        write_out,
        out_shape=(
            jax.ShapeDtypeStruct((D, 128), BF16),
            jax.ShapeDtypeStruct((D, 128), BF16),
            jax.ShapeDtypeStruct((NZ, NX, 128, 128), BF16),
            jax.ShapeDtypeStruct((TOK, KB), BF16),
        ),
        in_specs=[vmem] * 4,
        out_specs=(hbm, hbm, hbm, hbm),
        scratch_shapes=[pltpu.VMEM((TOK, KB), BF16), dma((4,))],
        compiler_params=pltpu.CompilerParams(vmem_limit_bytes=6 * 2**20),
        name="write_out",
    )(*(pltpu.with_memory_space_constraint(a, pltpu.VMEM) for a in held))
    return (mixed, gate[None], up[None], down.reshape(1, D, 128))


def solution(mesh):
    in_specs = (
        P("fs", None),
        P("fs", None),
        P("fs", None),
        P("fs"),
        P(None, "fs", "tp"),
        P(None, "fs", "tp"),
        P(None, "fs", "tp"),
    )
    out_specs = (P("fs", "tp"), P("tp", None, "fs"), P("tp", None, "fs"), P("tp", None, "fs"))
    return jax.shard_map(
        per_device, mesh=mesh, in_specs=in_specs, out_specs=out_specs, check_vma=False
    )
```
